32 devices in a mesh: ep: 32 (over z, y, x, core).
Axes of the slice: x: 2, y: 2, z: 4, core: 2. Of those that a mesh axis runs over, the one named last changes fastest.
Arguments:
- tokens: bfloat16 [256, 2048], P('ep'), may hold values from -6 to 6
- premix_gain: float32 [2048], replicated, may hold values from 0.1 to 1.9
- postmix_gain: float32 [2048], replicated, may hold values from 0.1 to 1.9
- prefeed_gain: float32 [2048], replicated, may hold values from 0.1 to 1.9
- postfeed_gain: float32 [2048], replicated, may hold values from 0.1 to 1.9
- query_weight: bfloat16 [2048, 1024], P('ep'), may hold values from -0.125 to 0.125
- key_weight: bfloat16 [2048, 1024], P('ep'), may hold values from -0.125 to 0.125
- value_weight: bfloat16 [2048, 1024], P('ep'), may hold values from -0.125 to 0.125
- outgate_weight: bfloat16 [2048, 1024], P('ep'), may hold values from -0.125 to 0.125
- ingate_weight: bfloat16 [2048, 8], replicated, may hold values from -0.125 to 0.125
- forget_weight: bfloat16 [2048, 8], replicated, may hold values from -0.125 to 0.125
- ingate_bias: float32 [8], replicated, may hold values from -1 to 1
- forget_bias: float32 [8], replicated, may hold values from -1 to 5
- memory_state: float32 [256, 8, 128, 128], P('ep'), may hold values from -1.25 to 1.25
- normalizer: float32 [256, 8, 128], P('ep'), may hold values from -1.75 to 1.75
- stabilizer: float32 [256, 8], P('ep'), may hold values from -2 to 2
- output_weight: bfloat16 [1024, 2048], P(None, 'ep'), may hold values from -0.1875 to 0.1875
- expert_ids: int32 [256, 6], P('ep'), may hold values from 0 to 31, all different within a row; in each aligned block of 8 rows (0 to 7, 8 to 15, ...) at most 4 rows name the same one
- route_weights: float32 [256, 6], P('ep'), may hold values from 0.2 to 0.8
- expert_gate: bfloat16 [32, 2048, 512], P('ep'), may hold values from -0.125 to 0.125
- expert_up: bfloat16 [32, 2048, 512], P('ep'), may hold values from -0.125 to 0.125
- expert_down: bfloat16 [32, 512, 2048], P('ep'), may hold values from -0.25 to 0.25
- shared_gate: bfloat16 [2048, 512], replicated, may hold values from -0.125 to 0.125
- shared_up: bfloat16 [2048, 512], replicated, may hold values from -0.125 to 0.125
- shared_down: bfloat16 [512, 2048], replicated, may hold values from -0.25 to 0.25
Outputs:
- next_tokens: bfloat16 [256, 2048], P('ep')
- next_memory: float32 [256, 8, 128, 128], P('ep')
- next_normalizer: float32 [256, 8, 128], P('ep')
- next_stabilizer: float32 [256, 8], P('ep')
The draws below stay inside these ranges and needn't reach their ends.
Inputs may be any that keep to these rules, and one draw needn't show every extreme that they name: `expert_ids`: each row names 6 different experts. Among the rows of one device no expert is named more than 4 times, and in every draw some expert is named exactly 4 times by the rows of some device.
All inputs are finite; a program needn't handle non-finite values.
Results may differ from the reference program's by a relative error of at most 0.0097.
Values may be sent and summed in bfloat16 or wider, within the bound.
A program may use at most 128 MiB of HBM per device.

```python
import math
import jax
import jax.numpy as jnp
import numpy as np
from jax import lax

D = 2048
HEADS = 8
HEAD_DIM = 128
D_MEM = 1024
FF = 512
TOP_K = 6
EXPERTS = 32
SEQ_DEV = 8
SEQS = 256
CAP = 4
N_EP = 32


def block_scale(stream_key, extent, split, smallest, top_value):
    factor_of, own = 1.0, jax.random.fold_in(stream_key, 6)
    for axis_at, shards_of in split:
        heights = jnp.exp(jax.random.uniform(jax.random.fold_in(own, axis_at), (shards_of,), jnp.float32, smallest / len(split), top_value / len(split)))
        factor_of = factor_of * jnp.repeat(heights, extent[axis_at] // shards_of).reshape([-1 if axis == axis_at else 1 for axis in range(len(extent))])
    return factor_of


def deal_out(rng, own, number, rows, number_of, top, limit, slope):
    sequence = jax.random.permutation(rng, number_of)
    crowded, usual = portions_of(number_of, rows * top, limit, slope, True), portions_of(number_of, rows * top, limit, slope, False)
    places = jnp.arange(number_of)

    def named(lengths, rotation):
        used = int((lengths > 0).sum())
        fixed = max(1, used // 4)
        shifted = fixed + (places - fixed + rotation * (used - fixed)) % max(1, number_of - fixed)
        return jnp.zeros((number_of,), jnp.int32).at[sequence[jnp.where(places < fixed, places, shifted)]].set(jnp.asarray(lengths, jnp.int32))

    lengths = jnp.where(number % 4 == 0, named(crowded, number // 4), named(usual, number - number // 4 - 1))
    mixed = jax.random.permutation(jax.random.fold_in(own, 3), number_of)
    donor, taker = mixed[0:number_of // 2 * 2:2], mixed[1:number_of // 2 * 2:2]
    margin = jnp.minimum(lengths[donor] - 1, limit - lengths[taker]) // 2
    margin = jnp.where((donor == sequence[0]) | (taker == sequence[0]) | (lengths[taker] == 0), 0, jnp.maximum(margin, 0))
    shifted = jax.random.randint(jax.random.fold_in(own, 4), (number_of // 2,), 0, 1 << 20) % (margin + 1)
    lengths = lengths.at[donor].add(-shifted).at[taker].add(shifted)
    labels = jnp.searchsorted(jnp.cumsum(lengths), jnp.arange(rows * top), side="right").astype(jnp.int32)
    listing = labels.reshape(top, rows).T
    listing = listing[jax.random.permutation(jax.random.fold_in(own, 1), rows)]
    rotation = jax.random.randint(jax.random.fold_in(own, 2), (rows, 1), 0, top)
    return jnp.take_along_axis(listing, (jnp.arange(top)[None, :] + rotation) % top, axis=1)


def portions_of(number_of, total, limit, skew, full):
    weights = [(1 << 20) // math.isqrt(rank ** skew) + 1 for rank in range(1, number_of + 1)]
    largest = limit if full else min(limit, max(-(-total // number_of), total * weights[0] // sum(weights)))
    least = 1 if total - largest >= number_of - 1 else 0
    given, rest = [largest] + [least] * (number_of - 1), total - largest - least * (number_of - 1)
    while rest > 0:
        free = [i for i in range(1, number_of) if given[i] < largest] or [i for i in range(1, number_of) if given[i] < limit]
        pool, left = sum([weights[i] for i in free]), rest
        for i in free:
            addition = min(limit - given[i], max(1, left * weights[i] // pool), rest)
            given[i] = given[i] + addition
            rest = rest - addition
    return np.array(given)


def noise(own_key, extent, scale, bound, shards=(), kind=jnp.bfloat16):
    result = scale * jax.random.normal(own_key, extent, jnp.float32)
    if shards:
        result = result * block_scale(own_key, extent, shards, -0.22, 0.18)
    return jnp.clip(result, -bound, bound).astype(kind)


def setup_inputs(seed: int = 0) -> dict:
    streams_of = jax.random.split(jax.random.key(seed), 26)
    tokens = noise(streams_of[0], (SEQS, D), 1.0, 6.0, ((0, 32),))
    premix_gain = jnp.clip(1.0 + 0.18 * jax.random.normal(streams_of[1], (D,), jnp.float32), 0.1, 1.9)
    postmix_gain = jnp.clip(1.0 + 0.18 * jax.random.normal(streams_of[2], (D,), jnp.float32), 0.1, 1.9)
    prefeed_gain = jnp.clip(1.0 + 0.18 * jax.random.normal(streams_of[3], (D,), jnp.float32), 0.1, 1.9)
    postfeed_gain = jnp.clip(1.0 + 0.18 * jax.random.normal(streams_of[4], (D,), jnp.float32), 0.1, 1.9)
    query_weight = noise(streams_of[5], (D, D_MEM), D ** -0.5, 0.125, ((0, 32),))
    key_weight = noise(streams_of[6], (D, D_MEM), D ** -0.5, 0.125, ((0, 32),))
    value_weight = noise(streams_of[7], (D, D_MEM), D ** -0.5, 0.125, ((0, 32),))
    outgate_weight = noise(streams_of[8], (D, D_MEM), D ** -0.5, 0.125, ((0, 32),))
    ingate_weight = noise(streams_of[9], (D, HEADS), D ** -0.5, 0.125)
    forget_weight = noise(streams_of[10], (D, HEADS), D ** -0.5, 0.125)
    ingate_bias = jnp.clip(jax.random.uniform(streams_of[11], (HEADS,), jnp.float32, -1.0, 1.0), -1.0, 1.0)
    forget_bias = jnp.clip(jax.random.uniform(streams_of[12], (HEADS,), jnp.float32, -1.0, 5.0), -1.0, 5.0)
    memory_state = noise(streams_of[13], (SEQS, HEADS, HEAD_DIM, HEAD_DIM), 0.2, 1.25, ((0, 32),), jnp.float32)
    normalizer = noise(streams_of[14], (SEQS, HEADS, HEAD_DIM), 0.3, 1.75, ((0, 32),), jnp.float32)
    stabilizer = jnp.clip(jax.random.uniform(streams_of[15], (SEQS, HEADS), jnp.float32, -2.0, 2.0) * block_scale(streams_of[15], (SEQS, HEADS), ((0, 32),), -0.4, 0.0), -2.0, 2.0)
    output_weight = noise(streams_of[16], (D_MEM, D), D_MEM ** -0.5, 0.1875, ((1, 32),))
    expert_ids_keys = jax.random.split(jax.random.fold_in(streams_of[17], 1), SEQS // SEQ_DEV)
    expert_ids_turns = jax.random.permutation(jax.random.fold_in(streams_of[17], 3), SEQS // SEQ_DEV)
    expert_ids = jax.vmap(lambda own, number: deal_out(jax.random.fold_in(streams_of[17], 2), own, number, SEQ_DEV, EXPERTS, TOP_K, CAP, 2))(expert_ids_keys, expert_ids_turns).reshape((SEQS, TOP_K))
    route_weights = jnp.clip(0.2 + 0.6 * jax.random.uniform(streams_of[18], (SEQS, TOP_K), jnp.float32) ** block_scale(streams_of[18], (SEQS, TOP_K), ((0, 32),), -0.2, 0.2), 0.2, 0.8)
    expert_gate = noise(streams_of[19], (EXPERTS, D, FF), D ** -0.5, 0.125, ((0, 32),))
    expert_up = noise(streams_of[20], (EXPERTS, D, FF), D ** -0.5, 0.125, ((0, 32),))
    expert_down = noise(streams_of[21], (EXPERTS, FF, D), FF ** -0.5, 0.25, ((0, 32),))
    shared_gate = noise(streams_of[22], (D, FF), D ** -0.5, 0.125)
    shared_up = noise(streams_of[23], (D, FF), D ** -0.5, 0.125)
    shared_down = noise(streams_of[24], (FF, D), FF ** -0.5, 0.25)
    return dict(tokens=tokens, premix_gain=premix_gain, postmix_gain=postmix_gain, prefeed_gain=prefeed_gain, postfeed_gain=postfeed_gain, query_weight=query_weight, key_weight=key_weight, value_weight=value_weight, outgate_weight=outgate_weight, ingate_weight=ingate_weight, forget_weight=forget_weight, ingate_bias=ingate_bias, forget_bias=forget_bias, memory_state=memory_state, normalizer=normalizer, stabilizer=stabilizer, output_weight=output_weight, expert_ids=expert_ids, route_weights=route_weights, expert_gate=expert_gate, expert_up=expert_up, expert_down=expert_down, shared_gate=shared_gate, shared_up=shared_up, shared_down=shared_down)


epsilon = 1e-06

def rms_scale(values, gain_row):
    return values * lax.rsqrt(lax.optimization_barrier(jnp.mean(values * values, axis=-1, keepdims=True)) + epsilon) * gain_row

def rounded(values):
    return lax.optimization_barrier(values.astype(jnp.bfloat16))

def memory_step(queries, key_rows, value_rows, out_gate, input_pre, forget_pre, memory_state, normalizer, stabilizer):
    sequences = queries.shape[0]
    head_count = memory_state.shape[1]
    head_width = memory_state.shape[2]
    query_heads = queries.astype(jnp.float32).reshape(sequences, head_count, head_width)
    key_heads = key_rows.astype(jnp.float32).reshape(sequences, head_count, head_width) * head_width ** (-0.5)
    value_heads = value_rows.astype(jnp.float32).reshape(sequences, head_count, head_width)
    carried = jax.nn.log_sigmoid(forget_pre) + stabilizer
    next_stabilizer = jnp.maximum(carried, input_pre)
    keep_old = jnp.exp(carried - next_stabilizer)
    write_new = jnp.exp(input_pre - next_stabilizer)
    local_score = write_new * lax.optimization_barrier(jnp.sum(query_heads * key_heads, axis=-1))
    read_memory = jnp.einsum('shvk,shk->shv', memory_state, query_heads, precision=lax.Precision.HIGHEST)
    numerator = keep_old[..., None] * read_memory + local_score[..., None] * value_heads
    denominator = keep_old * lax.optimization_barrier(jnp.sum(normalizer * query_heads, axis=-1)) + local_score
    memory_read = numerator / jnp.maximum(jnp.abs(denominator), 1.0)[..., None]
    gated_out = (jax.nn.sigmoid(out_gate.astype(jnp.float32)) * memory_read.reshape(sequences, head_count * head_width)).astype(jnp.bfloat16)
    next_memory = keep_old[..., None, None] * memory_state + write_new[..., None, None] * value_heads[..., :, None] * key_heads[..., None, :]
    next_normalizer = keep_old[..., None] * normalizer + write_new[..., None] * key_heads
    return (gated_out, next_memory, next_normalizer, next_stabilizer)

def expert_rows(row_block, gate_weight, up_weight, down_weight):
    gate_values = jnp.dot(row_block, gate_weight, preferred_element_type=jnp.float32)
    up_values = jnp.dot(row_block, up_weight, preferred_element_type=jnp.float32)
    inner_rows = (jax.nn.silu(gate_values) * up_values).astype(jnp.bfloat16)
    return jnp.dot(inner_rows, down_weight, preferred_element_type=jnp.float32)

def reference(tokens, premix_gain, postmix_gain, prefeed_gain, postfeed_gain, query_weight, key_weight, value_weight, outgate_weight, ingate_weight, forget_weight, ingate_bias, forget_bias, memory_state, normalizer, stabilizer, output_weight, expert_ids, route_weights, expert_gate, expert_up, expert_down, shared_gate, shared_up, shared_down):
    residual = tokens.astype(jnp.float32)
    normed = rms_scale(residual, premix_gain).astype(jnp.bfloat16)
    queries = rounded(jnp.dot(normed, query_weight, preferred_element_type=jnp.float32))
    key_rows = rounded(jnp.dot(normed, key_weight, preferred_element_type=jnp.float32))
    value_rows = rounded(jnp.dot(normed, value_weight, preferred_element_type=jnp.float32))
    out_gate = rounded(jnp.dot(normed, outgate_weight, preferred_element_type=jnp.float32))
    input_pre = jnp.dot(normed, ingate_weight, preferred_element_type=jnp.float32) + ingate_bias
    forget_pre = jnp.dot(normed, forget_weight, preferred_element_type=jnp.float32) + forget_bias
    gated_out, next_memory, next_normalizer, next_stabilizer = memory_step(queries, key_rows, value_rows, out_gate, input_pre, forget_pre, memory_state, normalizer, stabilizer)
    mixed = rounded(jnp.dot(gated_out, output_weight, preferred_element_type=jnp.float32))
    after_mix = rounded(residual + rms_scale(mixed.astype(jnp.float32), postmix_gain))
    after_float = after_mix.astype(jnp.float32)
    expert_input = rms_scale(after_float, prefeed_gain).astype(jnp.bfloat16)
    flat_ids = expert_ids.reshape(-1).astype(jnp.int32)
    one_hot = (flat_ids[:, None] == jnp.arange(EXPERTS, dtype=jnp.int32)[None, :]).astype(jnp.int32)
    earlier = jnp.cumsum(one_hot, axis=0) - one_hot
    slot_ids = lax.optimization_barrier(jnp.sum(earlier * one_hot, axis=1)).astype(jnp.int32)
    token_index = (jnp.arange(SEQS * TOP_K, dtype=jnp.int32) // TOP_K).astype(jnp.int32)
    slot_table = jnp.zeros((EXPERTS, N_EP * CAP), jnp.int32).at[flat_ids, slot_ids].set(token_index)

    def one_expert(inputs):
        rows_index, gate_weight, up_weight, down_weight = inputs
        return expert_rows(expert_input[rows_index], gate_weight, up_weight, down_weight).astype(jnp.bfloat16)
    outputs = lax.map(one_expert, (slot_table, expert_gate, expert_up, expert_down))
    picked = outputs[flat_ids, slot_ids].astype(jnp.float32).reshape(SEQS, TOP_K, D)
    routed = lax.optimization_barrier(jnp.sum(picked * route_weights[:, :, None], axis=1))
    shared_out = expert_rows(expert_input, shared_gate, shared_up, shared_down)
    next_tokens = (after_float + rms_scale(routed + shared_out, postfeed_gain)).astype(jnp.bfloat16)
    return (next_tokens, next_memory, next_normalizer, next_stabilizer)
```

```python
import functools

import jax
import jax.numpy as jnp
from jax import lax
from jax.experimental import pallas as pl
from jax.experimental.pallas import tpu as pltpu
from jax.sharding import PartitionSpec as P

epsilon = 1e-06
LANES = 128
GROUPS = 4
MESH = pl.DeviceIdType.MESH
VM = pl.BlockSpec(memory_space=pltpu.VMEM)
ANY = pl.BlockSpec(memory_space=pl.ANY)


def rms_scale(values, gain_row):
    return (
        values * lax.rsqrt(jnp.mean(values * values, axis=-1, keepdims=True) + epsilon) * gain_row
    )


def greet(n, me):
    sem = pltpu.get_barrier_semaphore()

    def signal(i, carry):
        pl.semaphore_signal(
            sem, inc=1, device_id=(lax.rem(me + i, n),), device_id_type=MESH
        )
        return carry

    lax.fori_loop(1, n, signal, 0)


def greeted(n):
    pl.semaphore_wait(pltpu.get_barrier_semaphore(), n - 1)


def send(src, dst, send_sem, recv_sem, peer):
    pltpu.make_async_remote_copy(
        src_ref=src,
        dst_ref=dst,
        send_sem=send_sem,
        recv_sem=recv_sem,
        device_id=(peer,),
        device_id_type=MESH,
    ).start()


def drain(ref, sem):
    pltpu.make_async_copy(ref, ref, sem).wait()


def routing(ids, route_weights, slot_count, capacity):
    sequences, choices = ids.shape
    slot = lax.broadcasted_iota(jnp.int32, (sequences, slot_count), 1).astype(jnp.float32)
    owner = jnp.floor((slot + 0.5) * (1.0 / capacity))
    turn = slot - owner * capacity
    chosen = jnp.zeros((sequences, slot_count), jnp.float32)
    weight_of = jnp.zeros((sequences, slot_count), jnp.float32)
    float_ids = ids.astype(jnp.float32)
    for choice in range(choices):
        same = float_ids[:, choice : choice + 1] == owner
        chosen = jnp.where(same, 1.0, chosen)
        weight_of = jnp.where(same, route_weights[:, choice : choice + 1], weight_of)
    earlier = jnp.zeros((sequences, slot_count), jnp.float32)
    row = lax.broadcasted_iota(jnp.int32, (sequences, slot_count), 0)
    for other in range(sequences - 1):
        earlier = earlier + jnp.where(row > other, chosen[other : other + 1], 0.0)
    slots = jnp.where(earlier == turn, chosen, 0.0)
    return slots, slots * weight_of


def across(left, right):
    return lax.dot_general(
        left, right, (((1,), (1,)), ((), ())), preferred_element_type=jnp.float32
    )


def two_layer(rows, gate_weight, up_weight, down_weight):
    gate_values = jnp.dot(rows, gate_weight, preferred_element_type=jnp.float32)
    up_values = jnp.dot(rows, up_weight, preferred_element_type=jnp.float32)
    inner_rows = (gate_values * jax.nn.sigmoid(gate_values) * up_values).astype(jnp.bfloat16)
    return jnp.dot(inner_rows, down_weight, preferred_element_type=jnp.float32)


def layer_kernel(n, groups, *refs):
    (
        tokens_ref,
        premix_ref,
        postmix_ref,
        prefeed_ref,
        postfeed_ref,
        input_bias_ref,
        forget_bias_ref,
        normalizer_ref,
        stabilizer_ref,
        ids_ref,
        route_ref,
        mix_ref,
        query_ref,
        key_ref,
        value_ref,
        gate_ref,
    ) = refs[:16]
    loads_from = refs[16:25]
    out_ref, next_memory_ref, next_normalizer_ref, next_stabilizer_ref = refs[25:29]
    loaded = refs[29:38]
    (
        normed_buf,
        rows_buf,
        weight_buf,
        product_buf,
        result_buf,
        mix_buf,
        split_buf,
        gated_src,
        gated_buf,
        columns_buf,
        mixed_buf,
        outgoing,
        arrived,
        answer,
        returned,
        projected_ref,
        gates_ref,
        load_sems,
        send_sems,
        recv_sems,
    ) = refs[38:]
    weights = loaded[:6]
    input_weight, forget_weight, memory = loaded[6:]
    me = lax.axis_index("ep")
    members = n // groups
    plane, place = me // members, lax.rem(me, members)
    chips, near_chips = n // 2, members // 2
    chip, core, near_chip = me // 2, lax.rem(me, 2), place // 2
    partner = me + 1 - 2 * core
    part_width = rows_buf.shape[3]
    columns = weight_buf.shape[2]
    per_matrix = query_ref.shape[1] // columns
    greet(n, me)
    projections = (query_ref, key_ref, value_ref, gate_ref)

    def column(block):
        return pl.ds(pl.multiple_of(lax.rem(block, per_matrix) * columns, LANES), columns)

    for index, ref in enumerate(projections):

        @pl.when(place // per_matrix == index)
        def _():
            pltpu.make_async_copy(
                ref.at[:, column(place)], weight_buf.at[place], recv_sems.at[1]
            ).start()

    pltpu.make_async_copy(mix_ref, mix_buf.at[near_chip, core], recv_sems.at[3]).start()
    loads = [
        pltpu.make_async_copy(source, target, load_sems.at[index])
        for index, (source, target) in enumerate(zip(loads_from, loaded))
    ]
    residual = tokens_ref[...].astype(jnp.float32)
    normed = rms_scale(residual, premix_ref[...]).astype(jnp.bfloat16)
    for group in range(groups):
        normed_buf[group] = normed[:, group * part_width : (group + 1) * part_width]
    pltpu.make_async_copy(
        normed_buf.at[plane], rows_buf.at[chip, core], recv_sems.at[0]
    ).start()
    greeted(n)

    def send_rows(i, carry):
        peer = lax.rem(me + 2 * i, n)
        send(
            normed_buf.at[peer // members],
            rows_buf.at[chip, core],
            send_sems.at[0],
            recv_sems.at[0],
            peer,
        )
        return carry

    def send_weights(i, carry):
        block = lax.rem(place + i, members)
        for index, ref in enumerate(projections):

            @pl.when(block // per_matrix == index)
            def _():
                send(
                    ref.at[:, column(block)],
                    weight_buf.at[place],
                    send_sems.at[1],
                    recv_sems.at[1],
                    plane * members + block,
                )

        return carry

    lax.fori_loop(1, chips, send_rows, 0)
    lax.fori_loop(1, members, send_weights, 0)
    for index in (6, 7, 8, 3, 4, 5, 0, 1, 2):
        loads[index].start()

    loads[6].wait()
    loads[7].wait()
    input_pre = (
        across(normed, input_weight[...])
        + input_bias_ref[...]
    )
    forget_pre = (
        across(normed, forget_weight[...])
        + forget_bias_ref[...]
    )
    carried = (
        jnp.minimum(forget_pre, 0.0)
        - jnp.log1p(jnp.exp(-jnp.abs(forget_pre)))
        + stabilizer_ref[...]
    )
    next_stabilizer = jnp.maximum(carried, input_pre)
    keep_old = jnp.exp(carried - next_stabilizer)
    write_new = jnp.exp(input_pre - next_stabilizer)
    gates_ref[0] = keep_old
    gates_ref[1] = write_new
    next_stabilizer_ref[...] = next_stabilizer
    local, capacity, width = outgoing.shape[1:]
    slots, combine = routing(ids_ref[...], route_ref[...], n * local * capacity, capacity)
    dispatch = slots.T.astype(jnp.bfloat16)
    sequences, heads, head_width = memory.shape[:3]
    loads[8].wait()

    def split(s, carry):
        for head in range(heads):
            value = memory[s, head]
            high = value.astype(jnp.bfloat16)
            rows = pl.ds(pl.multiple_of(s * head_width, LANES), head_width)
            split_buf[head, rows, :head_width] = high
            split_buf[head, rows, head_width:] = (value - high.astype(jnp.float32)).astype(
                jnp.bfloat16
            )
        return carry

    lax.fori_loop(0, sequences, split, 0)

    drain(rows_buf.at[:, core], recv_sems.at[0])
    send(
        rows_buf.at[:, core], rows_buf.at[:, core], send_sems.at[8], recv_sems.at[8], partner
    )
    drain(weight_buf, recv_sems.at[1])
    drain(rows_buf.at[:, 1 - core], recv_sems.at[8])
    rows = rows_buf[...].reshape(n * rows_buf.shape[2], part_width)
    weight = weight_buf[...].reshape(weight_buf.shape[0] * weight_buf.shape[1], columns)
    product = jnp.dot(rows, weight, preferred_element_type=jnp.float32)
    product_buf[...] = product.reshape(product_buf.shape).astype(jnp.bfloat16)
    pltpu.make_async_copy(product_buf.at[me], result_buf.at[me], recv_sems.at[2]).start()

    def exchange(source, target, stage):
        def one(i, carry):
            peer = lax.rem(me + i, n)
            send(source.at[peer], target.at[me], send_sems.at[stage], recv_sems.at[stage], peer)
            return carry

        lax.fori_loop(1, n, one, 0)

    def send_mix(i, carry):
        send(
            mix_ref,
            mix_buf.at[near_chip, core],
            send_sems.at[3],
            recv_sems.at[3],
            plane * members + lax.rem(place + 2 * i, members),
        )
        return carry

    def line(source, target, stage):
        for i in range(1, groups):
            peer = lax.rem(plane + i, groups)
            send(
                source(peer),
                target.at[plane],
                send_sems.at[stage],
                recv_sems.at[stage],
                peer * members + place,
            )

    exchange(product_buf, result_buf, 2)
    lax.fori_loop(1, near_chips, send_mix, 0)
    drain(result_buf, recv_sems.at[2])
    for member in range(members):
        total = result_buf[member].astype(jnp.float32)
        for group in range(1, groups):
            total = total + result_buf[group * members + member].astype(jnp.float32)
        total = total.astype(jnp.bfloat16).astype(jnp.float32)
        projected_ref[:, member * columns : (member + 1) * columns] = total
    memory_width = heads * head_width
    row = lax.broadcasted_iota(jnp.int32, (sequences, head_width), 0)
    for head in range(heads):

        def piece(matrix):
            start = matrix * memory_width + head * head_width
            return projected_ref[:, start : start + head_width]

        span = slice(head * head_width, (head + 1) * head_width)
        query, value, out_gate = piece(0), piece(2), piece(3)
        key = piece(1) * head_width ** (-0.5)
        keep, write = keep_old[:, head : head + 1], write_new[:, head : head + 1]
        local_score = write * jnp.sum(query * key, axis=-1, keepdims=True)
        denominator = (
            keep * jnp.sum(normalizer_ref[:, head, :] * query, axis=-1, keepdims=True) + local_score
        )
        narrow = query.astype(jnp.bfloat16)
        reads = lax.dot_general(
            jnp.concatenate([narrow, narrow], axis=1),
            split_buf[head],
            (((1,), (1,)), ((), ())),
            preferred_element_type=jnp.float32,
        )
        read = jnp.zeros((sequences, head_width), jnp.float32)
        for s in range(sequences):
            read = jnp.where(row == s, reads[:, s * head_width : (s + 1) * head_width], read)
        memory_read = (keep * read + local_score * value) / jnp.maximum(
            jnp.abs(denominator), 1.0
        )
        gated_src[:, span] = (jax.nn.sigmoid(out_gate) * memory_read).astype(jnp.bfloat16)

    pltpu.make_async_copy(gated_src, gated_buf.at[plane], recv_sems.at[4]).start()
    line(lambda peer: gated_src, gated_buf, 4)
    drain(mix_buf.at[:, core], recv_sems.at[3])
    send(mix_buf.at[:, core], mix_buf.at[:, core], send_sems.at[9], recv_sems.at[9], partner)
    drain(gated_buf, recv_sems.at[4])
    drain(mix_buf.at[:, 1 - core], recv_sems.at[9])
    gated = gated_buf[...].reshape(gated_buf.shape[0] * gated_buf.shape[1], gated_buf.shape[2])
    mix_weight = mix_buf[...].reshape(members * mix_buf.shape[2], mix_buf.shape[3])
    columns_buf[...] = (
        lax.dot_general(
            gated, mix_weight, (((1,), (1,)), ((), ())), preferred_element_type=jnp.float32
        )
        .reshape(columns_buf.shape)
        .astype(jnp.bfloat16)
    )
    pltpu.make_async_copy(columns_buf.at[plane], mixed_buf.at[plane], recv_sems.at[5]).start()
    line(lambda peer: columns_buf.at[peer], mixed_buf, 5)
    drain(mixed_buf, recv_sems.at[5])
    mixed = jnp.concatenate([mixed_buf[group] for group in range(groups)], axis=1)
    after_mix = (residual + rms_scale(mixed.astype(jnp.float32), postmix_ref[...])).astype(
        jnp.bfloat16
    )
    after_float = after_mix.astype(jnp.float32)
    token_rows = rms_scale(after_float, prefeed_ref[...]).astype(jnp.bfloat16)
    outgoing[...] = (
        jnp.dot(dispatch, token_rows, preferred_element_type=jnp.float32)
        .reshape(outgoing.shape)
        .astype(jnp.bfloat16)
    )
    pltpu.make_async_copy(outgoing.at[me], arrived.at[me], recv_sems.at[6]).start()
    exchange(outgoing, arrived, 6)
    key_scale = head_width ** (-0.5)
    for head in range(heads):
        start = memory_width + head * head_width
        next_normalizer_ref[:, head, :] = keep_old[:, head : head + 1] * normalizer_ref[
            :, head, :
        ] + write_new[:, head : head + 1] * (
            projected_ref[:, start : start + head_width] * key_scale
        )

    def update(s, carry):
        line_of = pl.ds(s, 1)
        keep, write = gates_ref[0, line_of, :], gates_ref[1, line_of, :]
        keys = projected_ref[line_of, memory_width : 2 * memory_width] * key_scale
        values = projected_ref[line_of, 2 * memory_width : 3 * memory_width]
        stacked = jnp.concatenate(
            [
                write[:, head : head + 1] * values[:, head * head_width : (head + 1) * head_width]
                for head in range(heads)
            ],
            axis=0,
        ).T
        for head in range(heads):
            next_memory_ref[s, head] = (
                keep[:, head : head + 1] * memory[s, head]
                + stacked[:, head : head + 1]
                * keys[:, head * head_width : (head + 1) * head_width]
            )
        return carry

    lax.fori_loop(0, sequences, update, 0)
    for index in (3, 4, 5):
        loads[index].wait()
    shared_out = two_layer(token_rows, weights[3][...], weights[4][...], weights[5][...])
    for index in (0, 1, 2):
        loads[index].wait()
    drain(arrived, recv_sems.at[6])
    for item in range(local):
        block = arrived[:, item].astype(jnp.float32).reshape(n * capacity, width)
        answer[:, item] = (
            two_layer(
                block.astype(jnp.bfloat16),
                weights[0][item],
                weights[1][item],
                weights[2][item],
            )
            .reshape(n, capacity, width)
            .astype(jnp.bfloat16)
        )
    pltpu.make_async_copy(answer.at[me], returned.at[me], recv_sems.at[7]).start()
    exchange(answer, returned, 7)
    high = combine.astype(jnp.bfloat16)
    low = (combine - high.astype(jnp.float32)).astype(jnp.bfloat16)
    drain(returned, recv_sems.at[7])
    picked = (
        returned[...].astype(jnp.float32).reshape(combine.shape[1], width).astype(jnp.bfloat16)
    )
    combined = (
        shared_out
        + jnp.dot(high, picked, preferred_element_type=jnp.float32)
        + jnp.dot(low, picked, preferred_element_type=jnp.float32)
    )
    out_ref[...] = (after_float + rms_scale(combined, postfeed_ref[...])).astype(jnp.bfloat16)
    drain(rows_buf.at[pl.ds(0, chips - 1), 0], send_sems.at[0])
    drain(rows_buf.at[:, 0], send_sems.at[8])
    drain(weight_buf.at[pl.ds(0, members - 1)], send_sems.at[1])
    drain(result_buf.at[pl.ds(0, n - 1)], send_sems.at[2])
    drain(mix_buf.at[pl.ds(0, near_chips - 1), 0], send_sems.at[3])
    drain(mix_buf.at[:, 0], send_sems.at[9])
    drain(gated_buf.at[pl.ds(0, groups - 1)], send_sems.at[4])
    drain(mixed_buf.at[pl.ds(0, groups - 1)], send_sems.at[5])
    drain(arrived.at[pl.ds(0, n - 1)], send_sems.at[6])
    drain(returned.at[pl.ds(0, n - 1)], send_sems.at[7])


def layer(n, groups, small, projections, loads, capacity):
    tokens, mix_weight = small[0], small[-1]
    sequences, width = tokens.shape
    depth, columns = projections[0].shape
    members = n // groups
    wide = 4 * columns // members
    local = loads[0].shape[0]
    heads, head_width = loads[8].shape[1:3]
    narrow = functools.partial(pltpu.VMEM, dtype=jnp.bfloat16)
    slots = narrow((n, local, capacity, width))
    pieces = narrow((groups, sequences, width // groups))
    return pl.pallas_call(
        functools.partial(layer_kernel, n, groups),
        out_shape=(
            pltpu.VMEM((sequences, width), jnp.bfloat16),
            pltpu.VMEM(loads[8].shape, jnp.float32),
            pltpu.VMEM((sequences, heads, head_width), jnp.float32),
            pltpu.VMEM((sequences, heads), jnp.float32),
        ),
        in_specs=[VM] * len(small) + [ANY] * (len(projections) + len(loads)),
        out_specs=(VM,) * 4,
        scratch_shapes=[pltpu.VMEM(w.shape, w.dtype) for w in loads]
        + [
            pieces,
            narrow((n // 2, 2, sequences, width // groups)),
            narrow((members, depth, wide)),
            narrow((n, sequences, wide)),
            narrow((n, sequences, wide)),
            narrow((members // 2, 2) + mix_weight.shape),
            narrow((heads, sequences * head_width, 2 * head_width)),
            narrow((sequences, columns)),
            narrow((groups, sequences, columns)),
            pieces,
            pieces,
        ]
        + [slots] * 4
        + [
            pltpu.VMEM((sequences, 4 * columns), jnp.float32),
            pltpu.VMEM((2, sequences, heads), jnp.float32),
            pltpu.SemaphoreType.DMA((len(loads),)),
            pltpu.SemaphoreType.DMA((10,)),
            pltpu.SemaphoreType.DMA((10,)),
        ],
        compiler_params=pltpu.CompilerParams(
            collective_id=0, has_side_effects=True, vmem_limit_bytes=54 * 1024 * 1024
        ),
    )(
        *small,
        *[pltpu.with_memory_space_constraint(w, pltpu.HBM) for w in projections + loads],
    )


def publish_kernel(*refs):
    count = len(refs) // 2
    sems = refs[-1]
    copies = [
        pltpu.make_async_copy(refs[index], refs[count + index], sems.at[index])
        for index in range(count)
    ]
    for copy in copies:
        copy.start()
    for copy in copies:
        copy.wait()


def publish(*results):
    held = [pltpu.with_memory_space_constraint(result, pltpu.VMEM) for result in results]
    return pl.pallas_call(
        publish_kernel,
        out_shape=tuple(jax.ShapeDtypeStruct(r.shape, r.dtype) for r in results),
        in_specs=[VM] * len(results),
        out_specs=(ANY,) * len(results),
        scratch_shapes=[pltpu.SemaphoreType.DMA((len(results),))],
        compiler_params=pltpu.CompilerParams(vmem_limit_bytes=1024 * 1024),
    )(*held)


def on_device(
    tokens,
    premix_gain,
    postmix_gain,
    prefeed_gain,
    postfeed_gain,
    query_weight,
    key_weight,
    value_weight,
    outgate_weight,
    ingate_weight,
    forget_weight,
    ingate_bias,
    forget_bias,
    memory_state,
    normalizer,
    stabilizer,
    output_weight,
    expert_ids,
    route_weights,
    expert_gate,
    expert_up,
    expert_down,
    shared_gate,
    shared_up,
    shared_down,
):
    sequences = tokens.shape[0]
    devices = lax.axis_size("ep")
    experts_total = expert_gate.shape[0] * devices
    choose_count = expert_ids.shape[1]
    capacity = min(
        sequences, max(2, 2 * ((sequences * choose_count + experts_total - 1) // experts_total))
    )
    results = layer(
        devices,
        GROUPS,
        (
            tokens,
            premix_gain[None],
            postmix_gain[None],
            prefeed_gain[None],
            postfeed_gain[None],
            ingate_bias[None],
            forget_bias[None],
            normalizer,
            stabilizer,
            expert_ids,
            route_weights,
            output_weight.T,
        ),
        (query_weight, key_weight, value_weight, outgate_weight),
        (
            expert_gate,
            expert_up,
            expert_down,
            shared_gate,
            shared_up,
            shared_down,
            ingate_weight.T,
            forget_weight.T,
            memory_state,
        ),
        capacity,
    )
    return publish(*results)


def solution(mesh):
    in_specs = (
        P("ep", None),
        P(),
        P(),
        P(),
        P(),
        P("ep", None),
        P("ep", None),
        P("ep", None),
        P("ep", None),
        P(),
        P(),
        P(),
        P(),
        P("ep", None, None, None),
        P("ep", None, None),
        P("ep", None),
        P(None, "ep"),
        P("ep", None),
        P("ep", None),
        P("ep", None, None),
        P("ep", None, None),
        P("ep", None, None),
        P(),
        P(),
        P(),
    )
    out_specs = (P("ep", None), P("ep", None, None, None), P("ep", None, None), P("ep", None))
    return jax.shard_map(
        on_device, mesh=mesh, in_specs=in_specs, out_specs=out_specs, check_vma=False
    )
```

```python
import functools

import jax
import jax.numpy as jnp
from jax import lax
from jax.experimental import pallas as pl
from jax.experimental.pallas import tpu as pltpu
from jax.sharding import PartitionSpec as P

epsilon = 1e-06
LANES = 128
GROUPS = 4
FAR_IN = 3
FAR_OUT = 4
CUBE = 8
HALVES = 4
MESH = pl.DeviceIdType.MESH
VM = pl.BlockSpec(memory_space=pltpu.VMEM)
ANY = pl.BlockSpec(memory_space=pl.ANY)


def rms_scale(values, gain_row):
    return (
        values * lax.rsqrt(jnp.mean(values * values, axis=-1, keepdims=True) + epsilon) * gain_row
    )


def greet(n, me):
    sem = pltpu.get_barrier_semaphore()

    def signal(i, carry):
        pl.semaphore_signal(
            sem, inc=1, device_id=(lax.rem(me + i, n),), device_id_type=MESH
        )
        return carry

    lax.fori_loop(1, n, signal, 0)


def greeted(n):
    pl.semaphore_wait(pltpu.get_barrier_semaphore(), n - 1)


def send(src, dst, send_sem, recv_sem, peer):
    pltpu.make_async_remote_copy(
        src_ref=src,
        dst_ref=dst,
        send_sem=send_sem,
        recv_sem=recv_sem,
        device_id=(peer,),
        device_id_type=MESH,
    ).start()


def drain(ref, sem):
    pltpu.make_async_copy(ref, ref, sem).wait()


def flip(value, mask):
    result, bit = value, 1
    while bit <= mask:
        if mask & bit:
            result = result + bit * (1 - 2 * lax.rem(lax.div(value, bit), 2))
        bit *= 2
    return result


def routing(ids, route_weights, first_slot, slot_count, capacity):
    sequences, choices = ids.shape
    slot = (
        first_slot + lax.broadcasted_iota(jnp.int32, (sequences, slot_count), 1)
    ).astype(jnp.float32)
    owner = jnp.floor((slot + 0.5) * (1.0 / capacity))
    turn = slot - owner * capacity
    chosen = jnp.zeros((sequences, slot_count), jnp.float32)
    weight_of = jnp.zeros((sequences, slot_count), jnp.float32)
    float_ids = ids.astype(jnp.float32)
    for choice in range(choices):
        same = float_ids[:, choice : choice + 1] == owner
        chosen = jnp.where(same, 1.0, chosen)
        weight_of = jnp.where(same, route_weights[:, choice : choice + 1], weight_of)
    earlier = jnp.zeros((sequences, slot_count), jnp.float32)
    row = lax.broadcasted_iota(jnp.int32, (sequences, slot_count), 0)
    for other in range(sequences - 1):
        earlier = earlier + jnp.where(row > other, chosen[other : other + 1], 0.0)
    slots = jnp.where(earlier == turn, chosen, 0.0)
    return slots, slots * weight_of


def across(left, right):
    return lax.dot_general(
        left, right, (((1,), (1,)), ((), ())), preferred_element_type=jnp.float32
    )


def gated_rows(rows, gate_weight, up_weight):
    gate_values = jnp.dot(rows, gate_weight, preferred_element_type=jnp.float32)
    up_values = jnp.dot(rows, up_weight, preferred_element_type=jnp.float32)
    return (gate_values * jax.nn.sigmoid(gate_values) * up_values).astype(jnp.bfloat16)


def two_layer(rows, gate_weight, up_weight, down_weight):
    inner_rows = gated_rows(rows, gate_weight, up_weight)
    return jnp.dot(inner_rows, down_weight, preferred_element_type=jnp.float32)


def layer_kernel(n, groups, *refs):
    small_from = refs[:12]
    projections = refs[12:16]
    loads_from = refs[16:25]
    out_ref, next_memory_ref, next_normalizer_ref, next_stabilizer_ref = refs[25:29]
    small = refs[29:41]
    (
        tokens_ref,
        premix_ref,
        postmix_ref,
        prefeed_ref,
        postfeed_ref,
        input_bias_ref,
        forget_bias_ref,
        normalizer_ref,
        stabilizer_ref,
        ids_ref,
        route_ref,
        mix_ref,
    ) = small
    staged = refs[41]
    loaded = refs[42:51]
    (
        normed_buf,
        rows_buf,
        weight_buf,
        product_buf,
        result_buf,
        mix_buf,
        split_buf,
        gated_src,
        gated_buf,
        columns_buf,
        mixed_buf,
        outgoing,
        arrived,
        answer,
        returned,
        line_rows,
        near_out,
        near_in,
        near_answer,
        near_back,
        partial_out,
        partial_in,
        ids_line,
        route_line,
        dispatch_line,
        combine_line,
        projected_ref,
        gates_ref,
        small_sems,
        staged_sems,
        load_sems,
        send_sems,
        recv_sems,
        line_sems,
        weight_sems,
    ) = refs[51:]
    weights = loaded[:6]
    input_weight, forget_weight, memory = loaded[6:]
    me = lax.axis_index("ep")
    members = n // groups
    plane, place = me // members, lax.rem(me, members)
    chips, near_chips = n // 2, members // 2
    chip, core, near_chip = me // 2, lax.rem(me, 2), place // 2
    partner = me + 1 - 2 * core
    part_width = rows_buf.shape[3]
    halves, half_columns = weight_buf.shape[0], weight_buf.shape[3]
    columns = halves * half_columns
    per_matrix = staged.shape[2] // columns
    greet(n, me)
    small_loads = [
        pltpu.make_async_copy(source, target, small_sems.at[index])
        for index, (source, target) in enumerate(zip(small_from, small))
    ]
    staged_loads = [
        pltpu.make_async_copy(source, staged.at[index], staged_sems.at[index])
        for index, source in enumerate(projections)
    ]
    for copy in small_loads[:2] + staged_loads + small_loads[2:]:
        copy.start()
    cubes = members // CUBE
    UP, DOWN = range(groups), range(groups - 1, -1, -1)
    cube, corner = lax.div(place, CUBE), lax.rem(place, CUBE)

    def around(masks, body, include_own):
        def one(i, carry):
            base = lax.rem(cube + i, cubes) * CUBE
            for mask in masks:
                body(base + flip(corner, mask))
            return carry

        if not include_own:
            for mask in masks:
                if mask:
                    body(cube * CUBE + flip(corner, mask))
        lax.fori_loop(0 if include_own else 1, cubes, one, 0)

    def each_near(body, step=1):
        around(range(CUBE - step, -1, -step), body, False)

    def each_peer(body, step=1, order=range(groups - 1, -1, -1)):
        for mask in order:
            peers = flip(plane, mask)
            around(
                range(CUBE - step, -1, -step),
                lambda member: body(peers, member, peers * members + member),
                mask > 0,
            )
    def column(block, half):
        start = lax.rem(block, per_matrix) * columns + half * half_columns
        return pl.ds(pl.multiple_of(start, LANES), half_columns)

    loads = [
        pltpu.make_async_copy(source, target, load_sems.at[index])
        for index, (source, target) in enumerate(zip(loads_from, loaded))
    ]
    for copy in small_loads[:2]:
        copy.wait()
    residual = tokens_ref[...].astype(jnp.float32)
    normed = rms_scale(residual, premix_ref[...]).astype(jnp.bfloat16)
    for group in range(groups):
        normed_buf[group] = normed[:, group * part_width : (group + 1) * part_width]
    pltpu.make_async_copy(
        normed_buf.at[plane], rows_buf.at[chip, core], recv_sems.at[0]
    ).start()
    for copy in staged_loads + small_loads[2:]:
        copy.wait()
    for half in range(halves):
        pltpu.make_async_copy(
            staged.at[lax.div(place, per_matrix), :, column(place, half)],
            weight_buf.at[half, place],
            weight_sems.at[half],
        ).start()
    pltpu.make_async_copy(mix_ref, mix_buf.at[near_chip, core], recv_sems.at[3]).start()
    pltpu.make_async_copy(ids_ref, ids_line.at[plane], recv_sems.at[10]).start()
    pltpu.make_async_copy(route_ref, route_line.at[plane], recv_sems.at[11]).start()
    greeted(n)

    def send_rows(group, member, peer):
        send(
            normed_buf.at[group],
            rows_buf.at[chip, core],
            send_sems.at[0],
            recv_sems.at[0],
            peer,
        )

    def line(source, target, stage):
        for mask in range(groups - 1, 0, -1):
            peer = flip(plane, mask)
            send(
                source(peer),
                target.at[plane],
                send_sems.at[stage],
                recv_sems.at[stage],
                peer * members + place,
            )

    def send_weights(half):
        def one(block):
            send(
                staged.at[lax.div(block, per_matrix), :, column(block, half)],
                weight_buf.at[half, place],
                send_sems.at[1],
                weight_sems.at[half],
                plane * members + block,
            )

        each_near(one)

    each_peer(send_rows, 2)
    for half in range(halves):
        send_weights(half)
    line(lambda peer: ids_ref, ids_line, 10)
    line(lambda peer: route_ref, route_line, 11)
    for index in (6, 7, 8, 3, 4, 5, 0, 1, 2):
        loads[index].start()

    loads[6].wait()
    loads[7].wait()
    input_pre = (
        across(normed, input_weight[...])
        + input_bias_ref[...]
    )
    forget_pre = (
        across(normed, forget_weight[...])
        + forget_bias_ref[...]
    )
    carried = (
        jnp.minimum(forget_pre, 0.0)
        - jnp.log1p(jnp.exp(-jnp.abs(forget_pre)))
        + stabilizer_ref[...]
    )
    next_stabilizer = jnp.maximum(carried, input_pre)
    keep_old = jnp.exp(carried - next_stabilizer)
    write_new = jnp.exp(input_pre - next_stabilizer)
    gates_ref[0] = keep_old
    gates_ref[1] = write_new
    next_stabilizer_ref[...] = next_stabilizer
    local, capacity, far = outgoing.shape[1:]
    width = tokens_ref.shape[1]
    near = width - far
    slot_count = n * local * capacity
    near_slots = members * local * capacity
    slots, combine = routing(ids_ref[...], route_ref[...], 0, slot_count, capacity)
    dispatch = slots.T.astype(jnp.bfloat16)
    sequences, heads, head_width = memory.shape[:3]
    loads[8].wait()

    def split(s, carry):
        for head in range(heads):
            value = memory[s, head]
            high = value.astype(jnp.bfloat16)
            rows = pl.ds(pl.multiple_of(s * head_width, LANES), head_width)
            split_buf[head, rows, :head_width] = high
            split_buf[head, rows, head_width:] = (value - high.astype(jnp.float32)).astype(
                jnp.bfloat16
            )
        return carry

    lax.fori_loop(0, sequences, split, 0)

    def exchange(source, target, stage, order):
        def one(group, member, peer):
            send(source.at[peer], target.at[me], send_sems.at[stage], recv_sems.at[stage], peer)

        each_peer(one, 1, order)

    drain(rows_buf.at[:, core], recv_sems.at[0])
    send(
        rows_buf.at[:, core], rows_buf.at[:, core], send_sems.at[8], recv_sems.at[8], partner
    )
    for half in range(halves):
        drain(weight_buf.at[half], weight_sems.at[half])
        if half == 0:
            drain(rows_buf.at[:, 1 - core], recv_sems.at[8])
        rows = rows_buf[...].reshape(n * rows_buf.shape[2], part_width)
        weight = weight_buf[half].reshape(members * weight_buf.shape[2], half_columns)
        product = jnp.dot(rows, weight, preferred_element_type=jnp.float32)
        product_buf[half] = product.reshape(product_buf.shape[1:]).astype(jnp.bfloat16)
        pltpu.make_async_copy(
            product_buf.at[half, me], result_buf.at[half, me], recv_sems.at[2]
        ).start()
        exchange(product_buf.at[half], result_buf.at[half], 2, DOWN)

    def send_mix(member):
        send(
            mix_ref,
            mix_buf.at[near_chip, core],
            send_sems.at[3],
            recv_sems.at[3],
            plane * members + member,
        )

    each_near(send_mix, 2)
    drain(ids_line, recv_sems.at[10])
    drain(route_line, recv_sems.at[11])
    for group in range(groups):
        near_chosen, near_combine = routing(
            ids_line[group], route_line[group], plane * near_slots, near_slots, capacity
        )
        dispatch_line[group] = near_chosen.T.astype(jnp.bfloat16)
        near_high = near_combine.astype(jnp.bfloat16)
        combine_line[group, :sequences] = near_high
        combine_line[group, sequences:] = (
            near_combine - near_high.astype(jnp.float32)
        ).astype(jnp.bfloat16)
    drain(result_buf, recv_sems.at[2])
    for half in range(halves):
        for member in range(members):
            total = result_buf[half, member].astype(jnp.float32)
            for group in range(1, groups):
                total = total + result_buf[half, group * members + member].astype(jnp.float32)
            total = total.astype(jnp.bfloat16).astype(jnp.float32)
            start = member * columns + half * half_columns
            projected_ref[:, start : start + half_columns] = total
    memory_width = heads * head_width
    row = lax.broadcasted_iota(jnp.int32, (sequences, head_width), 0)
    for head in range(heads):

        def piece(matrix):
            start = matrix * memory_width + head * head_width
            return projected_ref[:, start : start + head_width]

        span = slice(head * head_width, (head + 1) * head_width)
        query, value, out_gate = piece(0), piece(2), piece(3)
        key = piece(1) * head_width ** (-0.5)
        keep, write = keep_old[:, head : head + 1], write_new[:, head : head + 1]
        local_score = write * jnp.sum(query * key, axis=-1, keepdims=True)
        denominator = (
            keep * jnp.sum(normalizer_ref[:, head, :] * query, axis=-1, keepdims=True) + local_score
        )
        narrow = query.astype(jnp.bfloat16)
        reads = lax.dot_general(
            jnp.concatenate([narrow, narrow], axis=1),
            split_buf[head],
            (((1,), (1,)), ((), ())),
            preferred_element_type=jnp.float32,
        )
        read = jnp.zeros((sequences, head_width), jnp.float32)
        for s in range(sequences):
            read = jnp.where(row == s, reads[:, s * head_width : (s + 1) * head_width], read)
        memory_read = (keep * read + local_score * value) / jnp.maximum(
            jnp.abs(denominator), 1.0
        )
        gated_src[:, span] = (jax.nn.sigmoid(out_gate) * memory_read).astype(jnp.bfloat16)

    pltpu.make_async_copy(gated_src, gated_buf.at[plane], recv_sems.at[4]).start()
    line(lambda peer: gated_src, gated_buf, 4)
    key_scale = head_width ** (-0.5)
    for head in range(heads):
        start = memory_width + head * head_width
        next_normalizer_ref[:, head, :] = keep_old[:, head : head + 1] * normalizer_ref[
            :, head, :
        ] + write_new[:, head : head + 1] * (
            projected_ref[:, start : start + head_width] * key_scale
        )

    def update(s, carry):
        line_of = pl.ds(s, 1)
        keep, write = gates_ref[0, line_of, :], gates_ref[1, line_of, :]
        keys = projected_ref[line_of, memory_width : 2 * memory_width] * key_scale
        values = projected_ref[line_of, 2 * memory_width : 3 * memory_width]
        stacked = jnp.concatenate(
            [
                write[:, head : head + 1] * values[:, head * head_width : (head + 1) * head_width]
                for head in range(heads)
            ],
            axis=0,
        ).T
        for head in range(heads):
            next_memory_ref[s, head] = (
                keep[:, head : head + 1] * memory[s, head]
                + stacked[:, head : head + 1]
                * keys[:, head * head_width : (head + 1) * head_width]
            )
        return carry

    lax.fori_loop(0, sequences // 2, update, 0)
    drain(mix_buf.at[:, core], recv_sems.at[3])
    send(mix_buf.at[:, core], mix_buf.at[:, core], send_sems.at[9], recv_sems.at[9], partner)
    drain(gated_buf, recv_sems.at[4])
    drain(mix_buf.at[:, 1 - core], recv_sems.at[9])
    gated = gated_buf[...].reshape(gated_buf.shape[0] * gated_buf.shape[1], gated_buf.shape[2])
    mix_weight = mix_buf[...].reshape(members * mix_buf.shape[2], mix_buf.shape[3])
    columns_buf[...] = (
        lax.dot_general(
            gated, mix_weight, (((1,), (1,)), ((), ())), preferred_element_type=jnp.float32
        )
        .reshape(columns_buf.shape)
        .astype(jnp.bfloat16)
    )
    pltpu.make_async_copy(columns_buf.at[plane], mixed_buf.at[plane], recv_sems.at[5]).start()
    line(lambda peer: columns_buf.at[peer], mixed_buf, 5)
    lax.fori_loop(sequences // 2, sequences, update, 0)
    drain(mixed_buf, recv_sems.at[5])
    mixed = jnp.concatenate([mixed_buf[group] for group in range(groups)], axis=1)
    after_mix = (residual + rms_scale(mixed.astype(jnp.float32), postmix_ref[...])).astype(
        jnp.bfloat16
    )
    after_float = after_mix.astype(jnp.float32)
    token_rows = rms_scale(after_float, prefeed_ref[...]).astype(jnp.bfloat16)
    line_rows[plane] = token_rows[:, far:]
    for mask in range(groups - 1, 0, -1):
        send(
            line_rows.at[plane],
            line_rows.at[plane],
            send_sems.at[12],
            line_sems.at[mask],
            flip(plane, mask) * members + place,
        )

    def deal(group):
        near_out[group] = (
            jnp.dot(
                dispatch_line[group], line_rows[group], preferred_element_type=jnp.float32
            )
            .reshape(near_out.shape[1:])
            .astype(jnp.bfloat16)
        )
        pltpu.make_async_copy(
            near_out.at[group, place], near_in.at[group, place], recv_sems.at[13]
        ).start()

        def one(member):
            send(
                near_out.at[group, member],
                near_in.at[group, place],
                send_sems.at[13],
                recv_sems.at[13],
                plane * members + member,
            )

        each_near(one)

    deal(plane)
    outgoing[...] = (
        jnp.dot(dispatch, token_rows[:, :far], preferred_element_type=jnp.float32)
        .reshape(outgoing.shape)
        .astype(jnp.bfloat16)
    )
    pltpu.make_async_copy(outgoing.at[me], arrived.at[me], recv_sems.at[6]).start()
    exchange(outgoing, arrived, 6, UP)
    for mask in range(1, groups):
        source = flip(plane, mask)
        drain(line_rows.at[source], line_sems.at[mask])
        deal(source)
    for index in (3, 4, 5):
        loads[index].wait()
    shared_out = two_layer(token_rows, weights[3][...], weights[4][...], weights[5][...])
    for index in (0, 1, 2):
        loads[index].wait()
    drain(near_in, recv_sems.at[13])
    drain(arrived, recv_sems.at[6])
    back = returned.shape[3]
    inner_rows = []
    for item in range(local):
        block = jnp.concatenate(
            [
                arrived[:, item].astype(jnp.float32).reshape(n * capacity, far),
                near_in[:, :, item].astype(jnp.float32).reshape(n * capacity, near),
            ],
            axis=1,
        ).astype(jnp.bfloat16)
        inner = gated_rows(block, weights[0][item], weights[1][item])
        inner_rows.append(inner)
        near_answer[:, :, item] = (
            jnp.dot(inner, weights[2][item, :, back:], preferred_element_type=jnp.float32)
            .reshape(groups, members, capacity, width - back)
            .astype(jnp.bfloat16)
        )
    pltpu.make_async_copy(
        near_answer.at[:, place], near_back.at[:, place], recv_sems.at[14]
    ).start()

    def send_back(member):
        send(
            near_answer.at[:, member],
            near_back.at[:, place],
            send_sems.at[14],
            recv_sems.at[14],
            plane * members + member,
        )

    each_near(send_back)
    for item in range(local):
        answer[:, item] = (
            jnp.dot(
                inner_rows[item], weights[2][item, :, :back], preferred_element_type=jnp.float32
            )
            .reshape(n, capacity, back)
            .astype(jnp.bfloat16)
        )
    pltpu.make_async_copy(answer.at[me], returned.at[me], recv_sems.at[7]).start()
    exchange(answer, returned, 7, DOWN)
    high = combine.astype(jnp.bfloat16)
    low = (combine - high.astype(jnp.float32)).astype(jnp.bfloat16)
    drain(near_back, recv_sems.at[14])

    def weigh(group):
        rows = near_back[group].astype(jnp.float32).reshape(near_slots, width - back)
        both = jnp.dot(
            combine_line[group], rows.astype(jnp.bfloat16), preferred_element_type=jnp.float32
        )
        return both[:sequences] + both[sequences:]

    for i in range(groups - 1, 0, -1):
        peer = flip(plane, i)
        partial_out[peer] = weigh(peer).astype(jnp.bfloat16)
        send(
            partial_out.at[peer],
            partial_in.at[i],
            send_sems.at[15],
            recv_sems.at[15],
            peer * members + place,
        )
    near_sum = shared_out[:, back:] + weigh(plane)
    drain(returned, recv_sems.at[7])
    picked = returned[...].astype(jnp.float32).reshape(slot_count, back).astype(jnp.bfloat16)
    far_sum = (
        shared_out[:, :back]
        + jnp.dot(high, picked, preferred_element_type=jnp.float32)
        + jnp.dot(low, picked, preferred_element_type=jnp.float32)
    )
    drain(partial_in.at[pl.ds(1, groups - 1)], recv_sems.at[15])
    for i in range(1, groups):
        near_sum = near_sum + partial_in[i].astype(jnp.float32)
    combined = jnp.concatenate([far_sum, near_sum], axis=1)
    out_ref[...] = (after_float + rms_scale(combined, postfeed_ref[...])).astype(jnp.bfloat16)
    drain(rows_buf.at[pl.ds(0, chips - 1), 0], send_sems.at[0])
    drain(rows_buf.at[:, 0], send_sems.at[8])
    drain(weight_buf.at[:, pl.ds(0, members - 1)], send_sems.at[1])
    drain(result_buf.at[:, pl.ds(0, n - 1)], send_sems.at[2])
    drain(mix_buf.at[pl.ds(0, near_chips - 1), 0], send_sems.at[3])
    drain(mix_buf.at[:, 0], send_sems.at[9])
    drain(gated_buf.at[pl.ds(0, groups - 1)], send_sems.at[4])
    drain(mixed_buf.at[pl.ds(0, groups - 1)], send_sems.at[5])
    drain(arrived.at[pl.ds(0, n - 1)], send_sems.at[6])
    drain(returned.at[pl.ds(0, n - 1)], send_sems.at[7])
    drain(ids_line.at[pl.ds(0, groups - 1)], send_sems.at[10])
    drain(route_line.at[pl.ds(0, groups - 1)], send_sems.at[11])
    drain(line_rows.at[pl.ds(0, groups - 1)], send_sems.at[12])
    drain(near_in.at[:, pl.ds(0, members - 1)], send_sems.at[13])
    drain(near_back.at[:, pl.ds(0, members - 1)], send_sems.at[14])
    drain(partial_in.at[pl.ds(0, groups - 1)], send_sems.at[15])


def layer(n, groups, small, projections, loads, capacity):
    tokens, mix_weight = small[0], small[-1]
    sequences, width = tokens.shape
    depth, columns = projections[0].shape
    members = n // groups
    wide = 4 * columns // members
    halves = max(1, min(HALVES, wide // LANES))
    local = loads[0].shape[0]
    heads, head_width = loads[8].shape[1:3]
    narrow = functools.partial(pltpu.VMEM, dtype=jnp.bfloat16)
    far = width * FAR_IN // 8 // LANES * LANES
    back = width * FAR_OUT // 8 // LANES * LANES
    near_slots = members * local * capacity

    def slots(size):
        return [narrow((n, local, capacity, size))] * 2

    def blocks(size):
        return [narrow((groups, members, local, capacity, size))] * 2

    def rows(size):
        return [narrow((groups, sequences, size))]

    choices = small[9].shape[1]
    pieces = narrow((groups, sequences, width // groups))
    return pl.pallas_call(
        functools.partial(layer_kernel, n, groups),
        out_shape=(
            pltpu.VMEM((sequences, width), jnp.bfloat16),
            pltpu.VMEM(loads[8].shape, jnp.float32),
            pltpu.VMEM((sequences, heads, head_width), jnp.float32),
            pltpu.VMEM((sequences, heads), jnp.float32),
        ),
        in_specs=[ANY] * (len(small) + len(projections) + len(loads)),
        out_specs=(VM,) * 4,
        scratch_shapes=[pltpu.VMEM(w.shape, w.dtype) for w in small]
        + [narrow((len(projections), depth, columns))]
        + [pltpu.VMEM(w.shape, w.dtype) for w in loads]
        + [
            pieces,
            narrow((n // 2, 2, sequences, width // groups)),
            narrow((halves, members, depth, wide // halves)),
            narrow((halves, n, sequences, wide // halves)),
            narrow((halves, n, sequences, wide // halves)),
            narrow((members // 2, 2) + mix_weight.shape),
            narrow((heads, sequences * head_width, 2 * head_width)),
            narrow((sequences, columns)),
            narrow((groups, sequences, columns)),
            pieces,
            pieces,
        ]
        + slots(far)
        + slots(back)
        + rows(width - far)
        + blocks(width - far)
        + blocks(width - back)
        + rows(width - back) * 2
        + [
            pltpu.VMEM((groups, sequences, choices), jnp.int32),
            pltpu.VMEM((groups, sequences, choices), jnp.float32),
            narrow((groups, near_slots, sequences)),
            narrow((groups, 2 * sequences, near_slots)),
            pltpu.VMEM((sequences, 4 * columns), jnp.float32),
            pltpu.VMEM((2, sequences, heads), jnp.float32),
            pltpu.SemaphoreType.DMA((len(small),)),
            pltpu.SemaphoreType.DMA((len(projections),)),
            pltpu.SemaphoreType.DMA((len(loads),)),
            pltpu.SemaphoreType.DMA((16,)),
            pltpu.SemaphoreType.DMA((16,)),
            pltpu.SemaphoreType.DMA((groups,)),
            pltpu.SemaphoreType.DMA((halves,)),
        ],
        compiler_params=pltpu.CompilerParams(
            collective_id=0, has_side_effects=True, vmem_limit_bytes=54 * 1024 * 1024
        ),
    )(
        *[
            pltpu.with_memory_space_constraint(w, pltpu.HBM)
            for w in small + projections + loads
        ],
    )


def publish_kernel(*refs):
    count = len(refs) // 2
    sems = refs[-1]
    copies = [
        pltpu.make_async_copy(refs[index], refs[count + index], sems.at[index])
        for index in range(count)
    ]
    for copy in copies:
        copy.start()
    for copy in copies:
        copy.wait()


def publish(*results):
    held = [pltpu.with_memory_space_constraint(result, pltpu.VMEM) for result in results]
    return pl.pallas_call(
        publish_kernel,
        out_shape=tuple(jax.ShapeDtypeStruct(r.shape, r.dtype) for r in results),
        in_specs=[VM] * len(results),
        out_specs=(ANY,) * len(results),
        scratch_shapes=[pltpu.SemaphoreType.DMA((len(results),))],
        compiler_params=pltpu.CompilerParams(vmem_limit_bytes=1024 * 1024),
    )(*held)


def on_device(
    tokens,
    premix_gain,
    postmix_gain,
    prefeed_gain,
    postfeed_gain,
    query_weight,
    key_weight,
    value_weight,
    outgate_weight,
    ingate_weight,
    forget_weight,
    ingate_bias,
    forget_bias,
    memory_state,
    normalizer,
    stabilizer,
    output_weight,
    expert_ids,
    route_weights,
    expert_gate,
    expert_up,
    expert_down,
    shared_gate,
    shared_up,
    shared_down,
):
    sequences = tokens.shape[0]
    devices = lax.axis_size("ep")
    experts_total = expert_gate.shape[0] * devices
    choose_count = expert_ids.shape[1]
    capacity = min(
        sequences, max(2, 2 * ((sequences * choose_count + experts_total - 1) // experts_total))
    )
    results = layer(
        devices,
        GROUPS,
        (
            tokens,
            premix_gain[None],
            postmix_gain[None],
            prefeed_gain[None],
            postfeed_gain[None],
            ingate_bias[None],
            forget_bias[None],
            normalizer,
            stabilizer,
            expert_ids,
            route_weights,
            output_weight.T,
        ),
        (query_weight, key_weight, value_weight, outgate_weight),
        (
            expert_gate,
            expert_up,
            expert_down,
            shared_gate,
            shared_up,
            shared_down,
            ingate_weight.T,
            forget_weight.T,
            memory_state,
        ),
        capacity,
    )
    return publish(*results)


def solution(mesh):
    in_specs = (
        P("ep", None),
        P(),
        P(),
        P(),
        P(),
        P("ep", None),
        P("ep", None),
        P("ep", None),
        P("ep", None),
        P(),
        P(),
        P(),
        P(),
        P("ep", None, None, None),
        P("ep", None, None),
        P("ep", None),
        P(None, "ep"),
        P("ep", None),
        P("ep", None),
        P("ep", None, None),
        P("ep", None, None),
        P("ep", None, None),
        P(),
        P(),
        P(),
    )
    out_specs = (P("ep", None), P("ep", None, None, None), P("ep", None, None), P("ep", None))
    return jax.shard_map(
        on_device, mesh=mesh, in_specs=in_specs, out_specs=out_specs, check_vma=False
    )
```

```python
import functools

import jax
import jax.numpy as jnp
from jax import lax
from jax.experimental import pallas as pl
from jax.experimental.pallas import tpu as pltpu
from jax.sharding import PartitionSpec as P

epsilon = 1e-06
LANES = 128
GROUPS = 4
FAR_IN = 3
FAR_OUT = 4
ROUNDS = 2
CORNERS_IN = None
CORNERS_OUT = range(8)
CUBE = 8
HALVES = 4
MESH = pl.DeviceIdType.MESH
VM = pl.BlockSpec(memory_space=pltpu.VMEM)
ANY = pl.BlockSpec(memory_space=pl.ANY)


def rms_scale(values, gain_row):
    return (
        values * lax.rsqrt(jnp.mean(values * values, axis=-1, keepdims=True) + epsilon) * gain_row
    )


def greet(n, me):
    sem = pltpu.get_barrier_semaphore()

    def signal(i, carry):
        pl.semaphore_signal(
            sem, inc=1, device_id=(lax.rem(me + i, n),), device_id_type=MESH
        )
        return carry

    lax.fori_loop(1, n, signal, 0)


def greeted(n):
    pl.semaphore_wait(pltpu.get_barrier_semaphore(), n - 1)


def send(src, dst, send_sem, recv_sem, peer):
    pltpu.make_async_remote_copy(
        src_ref=src,
        dst_ref=dst,
        send_sem=send_sem,
        recv_sem=recv_sem,
        device_id=(peer,),
        device_id_type=MESH,
    ).start()


def drain(ref, sem):
    pltpu.make_async_copy(ref, ref, sem).wait()


def flip(value, mask):
    result, bit = value, 1
    while bit <= mask:
        if mask & bit:
            result = result + bit * (1 - 2 * lax.rem(lax.div(value, bit), 2))
        bit *= 2
    return result


def routing(ids, route_weights, first_slot, slot_count, capacity, first_turn):
    sequences, choices = ids.shape
    slot = (
        first_slot + lax.broadcasted_iota(jnp.int32, (sequences, slot_count), 1)
    ).astype(jnp.float32)
    owner = jnp.floor((slot + 0.5) * (1.0 / capacity))
    turn = slot - owner * capacity + first_turn
    chosen = jnp.zeros((sequences, slot_count), jnp.float32)
    weight_of = jnp.zeros((sequences, slot_count), jnp.float32)
    float_ids = ids.astype(jnp.float32)
    for choice in range(choices):
        same = float_ids[:, choice : choice + 1] == owner
        chosen = jnp.where(same, 1.0, chosen)
        weight_of = jnp.where(same, route_weights[:, choice : choice + 1], weight_of)
    earlier = jnp.zeros((sequences, slot_count), jnp.float32)
    row = lax.broadcasted_iota(jnp.int32, (sequences, slot_count), 0)
    for other in range(sequences - 1):
        earlier = earlier + jnp.where(row > other, chosen[other : other + 1], 0.0)
    slots = jnp.where(earlier == turn, chosen, 0.0)
    return slots, slots * weight_of


def across(left, right):
    return lax.dot_general(
        left, right, (((1,), (1,)), ((), ())), preferred_element_type=jnp.float32
    )


def gated_rows(rows, gate_weight, up_weight):
    gate_values = jnp.dot(rows, gate_weight, preferred_element_type=jnp.float32)
    up_values = jnp.dot(rows, up_weight, preferred_element_type=jnp.float32)
    return (gate_values * jax.nn.sigmoid(gate_values) * up_values).astype(jnp.bfloat16)


def two_layer(rows, gate_weight, up_weight, down_weight):
    inner_rows = gated_rows(rows, gate_weight, up_weight)
    return jnp.dot(inner_rows, down_weight, preferred_element_type=jnp.float32)


def layer_kernel(n, groups, *refs):
    small_from = refs[:12]
    projections = refs[12:16]
    loads_from = refs[16:25]
    out_ref, next_memory_ref, next_normalizer_ref, next_stabilizer_ref = refs[25:29]
    small = refs[29:41]
    (
        tokens_ref,
        premix_ref,
        postmix_ref,
        prefeed_ref,
        postfeed_ref,
        input_bias_ref,
        forget_bias_ref,
        normalizer_ref,
        stabilizer_ref,
        ids_ref,
        route_ref,
        mix_ref,
    ) = small
    staged = refs[41]
    loaded = refs[42:51]
    (
        normed_buf,
        rows_buf,
        weight_buf,
        product_buf,
        result_buf,
        mix_buf,
        split_buf,
        gated_src,
        gated_buf,
        columns_buf,
        mixed_buf,
        outgoing,
        arrived,
        answer,
        returned,
        line_rows,
        near_out,
        near_in,
        near_answer,
        near_back,
        partial_out,
        partial_in,
        ids_line,
        route_line,
        dispatch_line,
        combine_line,
        near_sums,
        projected_ref,
        gates_ref,
        small_sems,
        staged_sems,
        load_sems,
        send_sems,
        recv_sems,
        line_sems,
        weight_sems,
        result_sems,
        mix_sems,
        near_sems,
        far_sems,
        back_sems,
        home_sems,
    ) = refs[51:]
    weights = loaded[:6]
    input_weight, forget_weight, memory = loaded[6:]
    me = lax.axis_index("ep")
    members = n // groups
    plane, place = me // members, lax.rem(me, members)
    chips, near_chips = n // 2, members // 2
    chip, core, near_chip = me // 2, lax.rem(me, 2), place // 2
    partner = me + 1 - 2 * core
    part_width = rows_buf.shape[3]
    halves, half_columns = weight_buf.shape[0], weight_buf.shape[3]
    columns = halves * half_columns
    per_matrix = staged.shape[2] // columns
    greet(n, me)
    small_loads = [
        pltpu.make_async_copy(source, target, small_sems.at[index])
        for index, (source, target) in enumerate(zip(small_from, small))
    ]
    staged_loads = [
        pltpu.make_async_copy(source, staged.at[index], staged_sems.at[index])
        for index, source in enumerate(projections)
    ]
    for copy in small_loads[:2] + staged_loads + small_loads[2:]:
        copy.start()
    cubes = members // CUBE
    UP, DOWN = range(groups), range(groups - 1, -1, -1)
    cube, corner = lax.div(place, CUBE), lax.rem(place, CUBE)

    def around(masks, body, include_own):
        def one(i, carry):
            base = lax.rem(cube + i, cubes) * CUBE
            for mask in masks:
                body(base + flip(corner, mask))
            return carry

        if not include_own:
            for mask in masks:
                if mask:
                    body(cube * CUBE + flip(corner, mask))
        lax.fori_loop(0 if include_own else 1, cubes, one, 0)

    def each_near(body, step=1):
        around(range(CUBE - step, -1, -step), body, False)

    def each_peer(body, step=1, order=range(groups - 1, -1, -1), corners=None):
        for mask in order:
            peers = flip(plane, mask)
            around(
                corners or range(CUBE - step, -1, -step),
                lambda member: body(peers, member, peers * members + member),
                mask > 0,
            )
    def column(block, half):
        start = lax.rem(block, per_matrix) * columns + half * half_columns
        return pl.ds(pl.multiple_of(start, LANES), half_columns)

    loads = [
        pltpu.make_async_copy(source, target, load_sems.at[index])
        for index, (source, target) in enumerate(zip(loads_from, loaded))
    ]
    for copy in small_loads[:2]:
        copy.wait()
    residual = tokens_ref[...].astype(jnp.float32)
    normed = rms_scale(residual, premix_ref[...]).astype(jnp.bfloat16)
    for group in range(groups):
        normed_buf[group] = normed[:, group * part_width : (group + 1) * part_width]
    pltpu.make_async_copy(
        normed_buf.at[plane], rows_buf.at[chip, core], recv_sems.at[0]
    ).start()
    for copy in staged_loads + small_loads[2:]:
        copy.wait()
    for half in range(halves):
        pltpu.make_async_copy(
            staged.at[lax.div(place, per_matrix), :, column(place, half)],
            weight_buf.at[half, place],
            weight_sems.at[half],
        ).start()
    pltpu.make_async_copy(mix_ref, mix_buf.at[near_chip, core], mix_sems.at[near_chip]).start()
    pltpu.make_async_copy(ids_ref, ids_line.at[plane], recv_sems.at[10]).start()
    pltpu.make_async_copy(route_ref, route_line.at[plane], recv_sems.at[11]).start()
    greeted(n)

    def send_rows(group, member, peer):
        send(
            normed_buf.at[group],
            rows_buf.at[chip, core],
            send_sems.at[0],
            recv_sems.at[0],
            peer,
        )

    def line(source, target, stage):
        for mask in range(groups - 1, 0, -1):
            peer = flip(plane, mask)
            send(
                source(peer),
                target.at[plane],
                send_sems.at[stage],
                recv_sems.at[stage],
                peer * members + place,
            )

    def send_weights(half):
        def one(block):
            send(
                staged.at[lax.div(block, per_matrix), :, column(block, half)],
                weight_buf.at[half, place],
                send_sems.at[1],
                weight_sems.at[half],
                plane * members + block,
            )

        each_near(one)

    each_peer(send_rows, 2)
    for half in range(halves):
        send_weights(half)
    line(lambda peer: ids_ref, ids_line, 10)
    line(lambda peer: route_ref, route_line, 11)
    for index in (6, 7, 8, 3, 4, 5, 0, 1, 2):
        loads[index].start()

    loads[6].wait()
    loads[7].wait()
    input_pre = (
        across(normed, input_weight[...])
        + input_bias_ref[...]
    )
    forget_pre = (
        across(normed, forget_weight[...])
        + forget_bias_ref[...]
    )
    carried = (
        jnp.minimum(forget_pre, 0.0)
        - jnp.log1p(jnp.exp(-jnp.abs(forget_pre)))
        + stabilizer_ref[...]
    )
    next_stabilizer = jnp.maximum(carried, input_pre)
    keep_old = jnp.exp(carried - next_stabilizer)
    write_new = jnp.exp(input_pre - next_stabilizer)
    gates_ref[0] = keep_old
    gates_ref[1] = write_new
    next_stabilizer_ref[...] = next_stabilizer
    rounds, _, local, capacity, far = outgoing.shape
    width = tokens_ref.shape[1]
    near = width - far
    slot_count = n * local * capacity
    near_slots = members * local * capacity
    dispatch, combine = [], []
    for turn in range(rounds):
        slots, combined = routing(
            ids_ref[...], route_ref[...], 0, slot_count, capacity, turn * capacity
        )
        dispatch.append(slots.T.astype(jnp.bfloat16))
        combine.append(combined)
    sequences, heads, head_width = memory.shape[:3]
    loads[8].wait()

    def split(s, carry):
        for head in range(heads):
            value = memory[s, head]
            high = value.astype(jnp.bfloat16)
            rows = pl.ds(pl.multiple_of(s * head_width, LANES), head_width)
            split_buf[head, rows, :head_width] = high
            split_buf[head, rows, head_width:] = (value - high.astype(jnp.float32)).astype(
                jnp.bfloat16
            )
        return carry

    lax.fori_loop(0, sequences, split, 0)

    def exchange(source, target, stage, order, corners=None, sem=None):
        def one(group, member, peer):
            send(source.at[peer], target.at[me], send_sems.at[stage], arrival, peer)

        arrival = recv_sems.at[stage] if sem is None else sem
        each_peer(one, 1, order, corners)

    drain(rows_buf.at[:, core], recv_sems.at[0])
    send(
        rows_buf.at[:, core], rows_buf.at[:, core], send_sems.at[8], recv_sems.at[8], partner
    )
    for half in range(halves):
        drain(weight_buf.at[half], weight_sems.at[half])
        if half == 0:
            drain(rows_buf.at[:, 1 - core], recv_sems.at[8])
        rows = rows_buf[...].reshape(n * rows_buf.shape[2], part_width)
        weight = weight_buf[half].reshape(members * weight_buf.shape[2], half_columns)
        product = jnp.dot(rows, weight, preferred_element_type=jnp.float32)
        product_buf[half] = product.reshape(product_buf.shape[1:]).astype(jnp.bfloat16)
        pltpu.make_async_copy(
            product_buf.at[half, me], result_buf.at[half, me], result_sems.at[half]
        ).start()
        exchange(
            product_buf.at[half], result_buf.at[half], 2, DOWN, None, result_sems.at[half]
        )

    def send_mix(member):
        send(
            mix_ref,
            mix_buf.at[near_chip, core],
            send_sems.at[3],
            mix_sems.at[near_chip],
            plane * members + member,
        )

    each_near(send_mix, 2)

    def forward_mix(member):
        index = lax.div(member, 2)
        drain(mix_buf.at[index, core], mix_sems.at[index])
        send(
            mix_buf.at[index, core],
            mix_buf.at[index, core],
            send_sems.at[9],
            recv_sems.at[9],
            partner,
        )

    forward_mix(place)
    drain(ids_line, recv_sems.at[10])
    drain(route_line, recv_sems.at[11])
    for turn in range(rounds):
        for group in range(groups):
            near_chosen, near_combine = routing(
                ids_line[group],
                route_line[group],
                plane * near_slots,
                near_slots,
                capacity,
                turn * capacity,
            )
            dispatch_line[turn, group] = near_chosen.T.astype(jnp.bfloat16)
            near_high = near_combine.astype(jnp.bfloat16)
            combine_line[turn, group, :sequences] = near_high
            combine_line[turn, group, sequences:] = (
                near_combine - near_high.astype(jnp.float32)
            ).astype(jnp.bfloat16)
    for half in range(halves):
        drain(result_buf.at[half], result_sems.at[half])
        for member in range(members):
            total = result_buf[half, member].astype(jnp.float32)
            for group in range(1, groups):
                total = total + result_buf[half, group * members + member].astype(jnp.float32)
            total = total.astype(jnp.bfloat16).astype(jnp.float32)
            start = member * columns + half * half_columns
            projected_ref[:, start : start + half_columns] = total
    memory_width = heads * head_width
    row = lax.broadcasted_iota(jnp.int32, (sequences, head_width), 0)
    for head in range(heads):

        def piece(matrix):
            start = matrix * memory_width + head * head_width
            return projected_ref[:, start : start + head_width]

        span = slice(head * head_width, (head + 1) * head_width)
        query, value, out_gate = piece(0), piece(2), piece(3)
        key = piece(1) * head_width ** (-0.5)
        keep, write = keep_old[:, head : head + 1], write_new[:, head : head + 1]
        local_score = write * jnp.sum(query * key, axis=-1, keepdims=True)
        denominator = (
            keep * jnp.sum(normalizer_ref[:, head, :] * query, axis=-1, keepdims=True) + local_score
        )
        narrow = query.astype(jnp.bfloat16)
        reads = lax.dot_general(
            jnp.concatenate([narrow, narrow], axis=1),
            split_buf[head],
            (((1,), (1,)), ((), ())),
            preferred_element_type=jnp.float32,
        )
        read = jnp.zeros((sequences, head_width), jnp.float32)
        for s in range(sequences):
            read = jnp.where(row == s, reads[:, s * head_width : (s + 1) * head_width], read)
        memory_read = (keep * read + local_score * value) / jnp.maximum(
            jnp.abs(denominator), 1.0
        )
        gated_src[:, span] = (jax.nn.sigmoid(out_gate) * memory_read).astype(jnp.bfloat16)

    pltpu.make_async_copy(gated_src, gated_buf.at[plane], recv_sems.at[4]).start()
    line(lambda peer: gated_src, gated_buf, 4)
    key_scale = head_width ** (-0.5)
    for head in range(heads):
        start = memory_width + head * head_width
        next_normalizer_ref[:, head, :] = keep_old[:, head : head + 1] * normalizer_ref[
            :, head, :
        ] + write_new[:, head : head + 1] * (
            projected_ref[:, start : start + head_width] * key_scale
        )

    def update(s, carry):
        line_of = pl.ds(s, 1)
        keep, write = gates_ref[0, line_of, :], gates_ref[1, line_of, :]
        keys = projected_ref[line_of, memory_width : 2 * memory_width] * key_scale
        values = projected_ref[line_of, 2 * memory_width : 3 * memory_width]
        stacked = jnp.concatenate(
            [
                write[:, head : head + 1] * values[:, head * head_width : (head + 1) * head_width]
                for head in range(heads)
            ],
            axis=0,
        ).T
        for head in range(heads):
            next_memory_ref[s, head] = (
                keep[:, head : head + 1] * memory[s, head]
                + stacked[:, head : head + 1]
                * keys[:, head * head_width : (head + 1) * head_width]
            )
        return carry

    lax.fori_loop(0, sequences // 2, update, 0)
    around(range(2, CUBE, 2), forward_mix, False)
    drain(gated_buf, recv_sems.at[4])
    drain(mix_buf.at[:, 1 - core], recv_sems.at[9])
    gated = gated_buf[...].reshape(gated_buf.shape[0] * gated_buf.shape[1], gated_buf.shape[2])
    mix_weight = mix_buf[...].reshape(members * mix_buf.shape[2], mix_buf.shape[3])
    columns_buf[...] = (
        lax.dot_general(
            gated, mix_weight, (((1,), (1,)), ((), ())), preferred_element_type=jnp.float32
        )
        .reshape(columns_buf.shape)
        .astype(jnp.bfloat16)
    )
    pltpu.make_async_copy(columns_buf.at[plane], mixed_buf.at[plane], recv_sems.at[5]).start()
    line(lambda peer: columns_buf.at[peer], mixed_buf, 5)
    lax.fori_loop(sequences // 2, sequences, update, 0)
    drain(mixed_buf, recv_sems.at[5])
    mixed = jnp.concatenate([mixed_buf[group] for group in range(groups)], axis=1)
    after_mix = (residual + rms_scale(mixed.astype(jnp.float32), postmix_ref[...])).astype(
        jnp.bfloat16
    )
    after_float = after_mix.astype(jnp.float32)
    token_rows = rms_scale(after_float, prefeed_ref[...]).astype(jnp.bfloat16)
    line_rows[plane] = token_rows[:, far:]
    for mask in range(groups - 1, 0, -1):
        send(
            line_rows.at[plane],
            line_rows.at[plane],
            send_sems.at[12],
            line_sems.at[mask],
            flip(plane, mask) * members + place,
        )

    def deal(turn, group):
        near_out[turn, group] = (
            jnp.dot(
                dispatch_line[turn, group], line_rows[group], preferred_element_type=jnp.float32
            )
            .reshape(near_out.shape[2:])
            .astype(jnp.bfloat16)
        )
        pltpu.make_async_copy(
            near_out.at[turn, group, place], near_in.at[turn, group, place], near_sems.at[turn]
        ).start()

        def one(member):
            send(
                near_out.at[turn, group, member],
                near_in.at[turn, group, place],
                send_sems.at[13],
                near_sems.at[turn],
                plane * members + member,
            )

        each_near(one)

    def deal_far(turn):
        outgoing[turn] = (
            jnp.dot(dispatch[turn], token_rows[:, :far], preferred_element_type=jnp.float32)
            .reshape(outgoing.shape[1:])
            .astype(jnp.bfloat16)
        )
        pltpu.make_async_copy(
            outgoing.at[turn, me], arrived.at[turn, me], far_sems.at[turn]
        ).start()
        exchange(
            outgoing.at[turn], arrived.at[turn], 6, UP, CORNERS_IN, far_sems.at[turn]
        )

    deal(0, plane)
    deal_far(0)
    for turn in range(1, rounds):
        deal(turn, plane)
    for mask in range(1, groups):
        source = flip(plane, mask)
        drain(line_rows.at[source], line_sems.at[mask])
        deal(0, source)
    for turn in range(1, rounds):
        deal_far(turn)
        for mask in range(1, groups):
            deal(turn, flip(plane, mask))
    for index in (3, 4, 5):
        loads[index].wait()
    shared_out = two_layer(token_rows, weights[3][...], weights[4][...], weights[5][...])
    for index in (0, 1, 2):
        loads[index].wait()
    back = returned.shape[4]
    near = width - far

    def work(turn):
        drain(near_in.at[turn], near_sems.at[turn])
        drain(arrived.at[turn], far_sems.at[turn])
        inner_rows = []
        for item in range(local):
            block = jnp.concatenate(
                [
                    arrived[turn, :, item].astype(jnp.float32).reshape(slot_count // local, far),
                    near_in[turn, :, :, item]
                    .astype(jnp.float32)
                    .reshape(slot_count // local, near),
                ],
                axis=1,
            ).astype(jnp.bfloat16)
            inner = gated_rows(block, weights[0][item], weights[1][item])
            inner_rows.append(inner)
            near_answer[turn, :, :, item] = (
                jnp.dot(inner, weights[2][item, :, back:], preferred_element_type=jnp.float32)
                .reshape(groups, members, capacity, width - back)
                .astype(jnp.bfloat16)
            )
        pltpu.make_async_copy(
            near_answer.at[turn, :, place], near_back.at[turn, :, place], back_sems.at[turn]
        ).start()

        def one(member):
            send(
                near_answer.at[turn, :, member],
                near_back.at[turn, :, place],
                send_sems.at[14],
                back_sems.at[turn],
                plane * members + member,
            )

        each_near(one)
        for item in range(local):
            answer[turn, :, item] = (
                jnp.dot(
                    inner_rows[item], weights[2][item, :, :back], preferred_element_type=jnp.float32
                )
                .reshape(n, capacity, back)
                .astype(jnp.bfloat16)
            )
        pltpu.make_async_copy(
            answer.at[turn, me], returned.at[turn, me], home_sems.at[turn]
        ).start()
        exchange(answer.at[turn], returned.at[turn], 7, DOWN, CORNERS_OUT, home_sems.at[turn])

    def weigh(turn, group):
        rows = near_back[turn, group].astype(jnp.float32).reshape(near_slots, width - back)
        both = jnp.dot(
            combine_line[turn, group], rows.astype(jnp.bfloat16), preferred_element_type=jnp.float32
        )
        return both[:sequences] + both[sequences:]

    def far_part(turn):
        drain(returned.at[turn], home_sems.at[turn])
        picked = returned[turn].astype(jnp.float32).reshape(slot_count, back).astype(jnp.bfloat16)
        high = combine[turn].astype(jnp.bfloat16)
        low = (combine[turn] - high.astype(jnp.float32)).astype(jnp.bfloat16)
        return jnp.dot(high, picked, preferred_element_type=jnp.float32) + jnp.dot(
            low, picked, preferred_element_type=jnp.float32
        )

    for turn in range(rounds):
        work(turn)
    last = rounds - 1
    far_sum = shared_out[:, :back]
    for turn in range(last):
        drain(near_back.at[turn], back_sems.at[turn])
        for i in range(groups):
            peer = flip(plane, i)
            known = weigh(turn, peer)
            near_sums[i] = known if turn == 0 else near_sums[i] + known
    drain(near_back.at[last], back_sems.at[last])
    for i in range(groups - 1, -1, -1):
        peer = flip(plane, i)
        total = weigh(last, peer)
        if last:
            total = total + near_sums[i]
        if i:
            partial_out[peer] = total.astype(jnp.bfloat16)
            send(
                partial_out.at[peer],
                partial_in.at[i],
                send_sems.at[15],
                recv_sems.at[15],
                peer * members + place,
            )
    near_sum = shared_out[:, back:] + total
    for turn in range(rounds):
        far_sum = far_sum + far_part(turn)
    drain(partial_in.at[pl.ds(1, groups - 1)], recv_sems.at[15])
    for i in range(1, groups):
        near_sum = near_sum + partial_in[i].astype(jnp.float32)
    combined = jnp.concatenate([far_sum, near_sum], axis=1)
    out_ref[...] = (after_float + rms_scale(combined, postfeed_ref[...])).astype(jnp.bfloat16)
    drain(rows_buf.at[pl.ds(0, chips - 1), 0], send_sems.at[0])
    drain(rows_buf.at[:, 0], send_sems.at[8])
    drain(weight_buf.at[:, pl.ds(0, members - 1)], send_sems.at[1])
    drain(result_buf.at[:, pl.ds(0, n - 1)], send_sems.at[2])
    drain(mix_buf.at[pl.ds(0, near_chips - 1), 0], send_sems.at[3])
    drain(mix_buf.at[:, 0], send_sems.at[9])
    drain(gated_buf.at[pl.ds(0, groups - 1)], send_sems.at[4])
    drain(mixed_buf.at[pl.ds(0, groups - 1)], send_sems.at[5])
    drain(arrived.at[:, pl.ds(0, n - 1)], send_sems.at[6])
    drain(returned.at[:, pl.ds(0, n - 1)], send_sems.at[7])
    drain(ids_line.at[pl.ds(0, groups - 1)], send_sems.at[10])
    drain(route_line.at[pl.ds(0, groups - 1)], send_sems.at[11])
    drain(line_rows.at[pl.ds(0, groups - 1)], send_sems.at[12])
    drain(near_in.at[:, :, pl.ds(0, members - 1)], send_sems.at[13])
    drain(near_back.at[:, :, pl.ds(0, members - 1)], send_sems.at[14])
    drain(partial_in.at[pl.ds(0, groups - 1)], send_sems.at[15])


def layer(n, groups, small, projections, loads, capacity):
    tokens, mix_weight = small[0], small[-1]
    sequences, width = tokens.shape
    depth, columns = projections[0].shape
    members = n // groups
    wide = 4 * columns // members
    halves = max(1, min(HALVES, wide // LANES))
    local = loads[0].shape[0]
    heads, head_width = loads[8].shape[1:3]
    narrow = functools.partial(pltpu.VMEM, dtype=jnp.bfloat16)
    far = width * FAR_IN // 8 // LANES * LANES
    back = width * FAR_OUT // 8 // LANES * LANES
    rounds = ROUNDS if capacity % (2 * ROUNDS) == 0 else 1
    capacity = capacity // rounds
    near_slots = members * local * capacity

    def slots(size):
        return [narrow((rounds, n, local, capacity, size))] * 2

    def blocks(size):
        return [narrow((rounds, groups, members, local, capacity, size))] * 2

    def rows(size):
        return [narrow((groups, sequences, size))]

    choices = small[9].shape[1]
    pieces = narrow((groups, sequences, width // groups))
    return pl.pallas_call(
        functools.partial(layer_kernel, n, groups),
        out_shape=(
            pltpu.VMEM((sequences, width), jnp.bfloat16),
            pltpu.VMEM(loads[8].shape, jnp.float32),
            pltpu.VMEM((sequences, heads, head_width), jnp.float32),
            pltpu.VMEM((sequences, heads), jnp.float32),
        ),
        in_specs=[ANY] * (len(small) + len(projections) + len(loads)),
        out_specs=(VM,) * 4,
        scratch_shapes=[pltpu.VMEM(w.shape, w.dtype) for w in small]
        + [narrow((len(projections), depth, columns))]
        + [pltpu.VMEM(w.shape, w.dtype) for w in loads]
        + [
            pieces,
            narrow((n // 2, 2, sequences, width // groups)),
            narrow((halves, members, depth, wide // halves)),
            narrow((halves, n, sequences, wide // halves)),
            narrow((halves, n, sequences, wide // halves)),
            narrow((members // 2, 2) + mix_weight.shape),
            narrow((heads, sequences * head_width, 2 * head_width)),
            narrow((sequences, columns)),
            narrow((groups, sequences, columns)),
            pieces,
            pieces,
        ]
        + slots(far)
        + slots(back)
        + rows(width - far)
        + blocks(width - far)
        + blocks(width - back)
        + rows(width - back) * 2
        + [
            pltpu.VMEM((groups, sequences, choices), jnp.int32),
            pltpu.VMEM((groups, sequences, choices), jnp.float32),
            narrow((rounds, groups, near_slots, sequences)),
            narrow((rounds, groups, 2 * sequences, near_slots)),
            pltpu.VMEM((groups, sequences, width - back), jnp.float32),
            pltpu.VMEM((sequences, 4 * columns), jnp.float32),
            pltpu.VMEM((2, sequences, heads), jnp.float32),
            pltpu.SemaphoreType.DMA((len(small),)),
            pltpu.SemaphoreType.DMA((len(projections),)),
            pltpu.SemaphoreType.DMA((len(loads),)),
            pltpu.SemaphoreType.DMA((18,)),
            pltpu.SemaphoreType.DMA((18,)),
            pltpu.SemaphoreType.DMA((groups,)),
            pltpu.SemaphoreType.DMA((halves,)),
            pltpu.SemaphoreType.DMA((halves,)),
            pltpu.SemaphoreType.DMA((members // 2,)),
            pltpu.SemaphoreType.DMA((rounds,)),
            pltpu.SemaphoreType.DMA((rounds,)),
            pltpu.SemaphoreType.DMA((rounds,)),
            pltpu.SemaphoreType.DMA((rounds,)),
        ],
        compiler_params=pltpu.CompilerParams(
            collective_id=0, has_side_effects=True, vmem_limit_bytes=54 * 1024 * 1024
        ),
    )(
        *[
            pltpu.with_memory_space_constraint(w, pltpu.HBM)
            for w in small + projections + loads
        ],
    )


def publish_kernel(*refs):
    count = len(refs) // 2
    sems = refs[-1]
    copies = [
        pltpu.make_async_copy(refs[index], refs[count + index], sems.at[index])
        for index in range(count)
    ]
    for copy in copies:
        copy.start()
    for copy in copies:
        copy.wait()


def publish(*results):
    held = [pltpu.with_memory_space_constraint(result, pltpu.VMEM) for result in results]
    return pl.pallas_call(
        publish_kernel,
        out_shape=tuple(jax.ShapeDtypeStruct(r.shape, r.dtype) for r in results),
        in_specs=[VM] * len(results),
        out_specs=(ANY,) * len(results),
        scratch_shapes=[pltpu.SemaphoreType.DMA((len(results),))],
        compiler_params=pltpu.CompilerParams(vmem_limit_bytes=1024 * 1024),
    )(*held)


def on_device(
    tokens,
    premix_gain,
    postmix_gain,
    prefeed_gain,
    postfeed_gain,
    query_weight,
    key_weight,
    value_weight,
    outgate_weight,
    ingate_weight,
    forget_weight,
    ingate_bias,
    forget_bias,
    memory_state,
    normalizer,
    stabilizer,
    output_weight,
    expert_ids,
    route_weights,
    expert_gate,
    expert_up,
    expert_down,
    shared_gate,
    shared_up,
    shared_down,
):
    sequences = tokens.shape[0]
    devices = lax.axis_size("ep")
    experts_total = expert_gate.shape[0] * devices
    choose_count = expert_ids.shape[1]
    capacity = min(
        sequences, max(2, 2 * ((sequences * choose_count + experts_total - 1) // experts_total))
    )
    results = layer(
        devices,
        GROUPS,
        (
            tokens,
            premix_gain[None],
            postmix_gain[None],
            prefeed_gain[None],
            postfeed_gain[None],
            ingate_bias[None],
            forget_bias[None],
            normalizer,
            stabilizer,
            expert_ids,
            route_weights,
            output_weight.T,
        ),
        (query_weight, key_weight, value_weight, outgate_weight),
        (
            expert_gate,
            expert_up,
            expert_down,
            shared_gate,
            shared_up,
            shared_down,
            ingate_weight.T,
            forget_weight.T,
            memory_state,
        ),
        capacity,
    )
    return publish(*results)


def solution(mesh):
    in_specs = (
        P("ep", None),
        P(),
        P(),
        P(),
        P(),
        P("ep", None),
        P("ep", None),
        P("ep", None),
        P("ep", None),
        P(),
        P(),
        P(),
        P(),
        P("ep", None, None, None),
        P("ep", None, None),
        P("ep", None),
        P(None, "ep"),
        P("ep", None),
        P("ep", None),
        P("ep", None, None),
        P("ep", None, None),
        P("ep", None, None),
        P(),
        P(),
        P(),
    )
    out_specs = (P("ep", None), P("ep", None, None, None), P("ep", None, None), P("ep", None))
    return jax.shard_map(
        on_device, mesh=mesh, in_specs=in_specs, out_specs=out_specs, check_vma=False
    )
```

```python
import functools

import jax
import jax.numpy as jnp
from jax import lax
from jax.experimental import pallas as pl
from jax.experimental.pallas import tpu as pltpu
from jax.sharding import PartitionSpec as P

epsilon = 1e-06
LANES = 128
GROUPS = 4
FAR_IN = 4
FAR_OUT = 4
ROUNDS = 2
CUBE = 8
HALVES = 4
MESH = pl.DeviceIdType.MESH
VM = pl.BlockSpec(memory_space=pltpu.VMEM)
ANY = pl.BlockSpec(memory_space=pl.ANY)


def rms_scale(values, gain_row):
    return (
        values * lax.rsqrt(jnp.mean(values * values, axis=-1, keepdims=True) + epsilon) * gain_row
    )


def greet(n, me):
    sem = pltpu.get_barrier_semaphore()

    def signal(i, carry):
        pl.semaphore_signal(
            sem, inc=1, device_id=(lax.rem(me + i, n),), device_id_type=MESH
        )
        return carry

    lax.fori_loop(1, n, signal, 0)


def greeted(n):
    pl.semaphore_wait(pltpu.get_barrier_semaphore(), n - 1)


def send(src, dst, send_sem, recv_sem, peer):
    pltpu.make_async_remote_copy(
        src_ref=src,
        dst_ref=dst,
        send_sem=send_sem,
        recv_sem=recv_sem,
        device_id=(peer,),
        device_id_type=MESH,
    ).start()


def drain(ref, sem):
    pltpu.make_async_copy(ref, ref, sem).wait()


def flip(value, mask):
    result, bit = value, 1
    while bit <= mask:
        if mask & bit:
            result = result + bit * (1 - 2 * lax.rem(lax.div(value, bit), 2))
        bit *= 2
    return result


def routing(ids, route_weights, first_slot, slot_count, capacity, first_turn):
    sequences, choices = ids.shape
    slot = (
        first_slot + lax.broadcasted_iota(jnp.int32, (sequences, slot_count), 1)
    ).astype(jnp.float32)
    owner = jnp.floor((slot + 0.5) * (1.0 / capacity))
    turn = slot - owner * capacity + first_turn
    chosen = jnp.zeros((sequences, slot_count), jnp.float32)
    weight_of = jnp.zeros((sequences, slot_count), jnp.float32)
    float_ids = ids.astype(jnp.float32)
    for choice in range(choices):
        same = float_ids[:, choice : choice + 1] == owner
        chosen = jnp.where(same, 1.0, chosen)
        weight_of = jnp.where(same, route_weights[:, choice : choice + 1], weight_of)
    earlier = jnp.zeros((sequences, slot_count), jnp.float32)
    row = lax.broadcasted_iota(jnp.int32, (sequences, slot_count), 0)
    for other in range(sequences - 1):
        earlier = earlier + jnp.where(row > other, chosen[other : other + 1], 0.0)
    slots = jnp.where(earlier == turn, chosen, 0.0)
    return slots, slots * weight_of


def across(left, right):
    return lax.dot_general(
        left, right, (((1,), (1,)), ((), ())), preferred_element_type=jnp.float32
    )


def gated_rows(rows, gate_weight, up_weight):
    gate_values = jnp.dot(rows, gate_weight, preferred_element_type=jnp.float32)
    up_values = jnp.dot(rows, up_weight, preferred_element_type=jnp.float32)
    return (gate_values * jax.nn.sigmoid(gate_values) * up_values).astype(jnp.bfloat16)


def two_layer(rows, gate_weight, up_weight, down_weight):
    inner_rows = gated_rows(rows, gate_weight, up_weight)
    return jnp.dot(inner_rows, down_weight, preferred_element_type=jnp.float32)


def layer_kernel(n, groups, *refs):
    small_from = refs[:12]
    projections = refs[12:16]
    loads_from = refs[16:25]
    out_ref, next_memory_ref, next_normalizer_ref, next_stabilizer_ref = refs[25:29]
    small = refs[29:41]
    (
        tokens_ref,
        premix_ref,
        postmix_ref,
        prefeed_ref,
        postfeed_ref,
        input_bias_ref,
        forget_bias_ref,
        normalizer_ref,
        stabilizer_ref,
        ids_ref,
        route_ref,
        mix_ref,
    ) = small
    staged = refs[41]
    loaded = refs[42:51]
    (
        normed_buf,
        rows_buf,
        weight_buf,
        product_buf,
        result_buf,
        mix_buf,
        split_buf,
        gated_src,
        gated_buf,
        columns_buf,
        mixed_buf,
        outgoing,
        arrived,
        answer,
        returned,
        line_rows,
        near_out,
        near_in,
        near_answer,
        near_back,
        partial_out,
        partial_in,
        ids_line,
        route_line,
        dispatch_line,
        combine_line,
        near_sums,
        projected_ref,
        gates_ref,
        sent,
        small_sems,
        staged_sem,
        load_sems,
        send_sem,
        route_sem,
        recv_sems,
        line_sems,
        weight_sems,
        result_sems,
        mix_sems,
        near_sems,
        far_sems,
        back_sems,
        home_sems,
    ) = refs[51:]
    weights = loaded[:6]
    input_weight, forget_weight, memory = loaded[6:]
    me = lax.axis_index("ep")
    members = n // groups
    plane, place = me // members, lax.rem(me, members)
    chips, near_chips = n // 2, members // 2
    chip, core, near_chip = me // 2, lax.rem(me, 2), place // 2
    partner = me + 1 - 2 * core
    part_width = rows_buf.shape[3]
    halves, half_columns = weight_buf.shape[0], weight_buf.shape[3]
    columns = halves * half_columns
    per_matrix = staged.shape[2] // columns
    greet(n, me)
    small_loads = [
        pltpu.make_async_copy(source, target, small_sems.at[index])
        for index, (source, target) in enumerate(zip(small_from, small))
    ]
    staged_loads = [
        pltpu.make_async_copy(source, staged.at[index], staged_sem)
        for index, source in enumerate(projections)
    ]
    for copy in small_loads[:2] + staged_loads + small_loads[2:]:
        copy.start()
    cubes = members // CUBE
    UP, DOWN = range(groups), range(groups - 1, -1, -1)
    cube, corner = lax.div(place, CUBE), lax.rem(place, CUBE)

    def around(masks, body, include_own):
        def one(i, carry):
            base = lax.rem(cube + i, cubes) * CUBE
            for mask in masks:
                body(base + flip(corner, mask))
            return carry

        if not include_own:
            for mask in masks:
                if mask:
                    body(cube * CUBE + flip(corner, mask))
        lax.fori_loop(0 if include_own else 1, cubes, one, 0)

    def each_near(body, step=1):
        around(range(CUBE - step, -1, -step), body, False)

    def each_peer(body, step=1, order=range(groups - 1, -1, -1), corners=None):
        for mask in order:
            peers = flip(plane, mask)
            around(
                corners or range(CUBE - step, -1, -step),
                lambda member: body(peers, member, peers * members + member),
                mask > 0,
            )
    def column(block, half):
        start = lax.rem(block, per_matrix) * columns + half * half_columns
        return pl.ds(pl.multiple_of(start, LANES), half_columns)

    loads = [
        pltpu.make_async_copy(source, target, load_sems.at[index])
        for index, (source, target) in enumerate(zip(loads_from, loaded))
    ]
    for copy in small_loads[:2]:
        copy.wait()
    residual = tokens_ref[...].astype(jnp.float32)
    normed = rms_scale(residual, premix_ref[...]).astype(jnp.bfloat16)
    for group in range(groups):
        normed_buf[group] = normed[:, group * part_width : (group + 1) * part_width]
    pltpu.make_async_copy(
        normed_buf.at[plane], rows_buf.at[chip, core], recv_sems.at[0]
    ).start()
    drain(staged, staged_sem)
    for copy in small_loads[2:]:
        copy.wait()
    greeted(n)

    def send_rows(group, member, peer):
        send(
            normed_buf.at[group],
            rows_buf.at[chip, core],
            send_sem,
            recv_sems.at[0],
            peer,
        )

    def line(source, target, stage, leave=None):
        for mask in range(groups - 1, 0, -1):
            peer = flip(plane, mask)
            send(
                source(peer),
                target.at[plane],
                send_sem if leave is None else leave,
                recv_sems.at[stage],
                peer * members + place,
            )

    def send_weights(half):
        def one(block):
            send(
                staged.at[lax.div(block, per_matrix), :, column(block, half)],
                weight_buf.at[half, place],
                send_sem,
                weight_sems.at[half],
                plane * members + block,
            )

        each_near(one)

    each_peer(send_rows, 2)
    for half in range(halves):
        send_weights(half)
    for half in range(halves):
        pltpu.make_async_copy(
            staged.at[lax.div(place, per_matrix), :, column(place, half)],
            weight_buf.at[half, place],
            weight_sems.at[half],
        ).start()
    pltpu.make_async_copy(mix_ref, mix_buf.at[near_chip, core], mix_sems.at[near_chip]).start()
    pltpu.make_async_copy(ids_ref, ids_line.at[plane], recv_sems.at[5]).start()
    pltpu.make_async_copy(route_ref, route_line.at[plane], recv_sems.at[6]).start()
    line(lambda peer: ids_ref, ids_line, 5, line_sems.at[0])
    line(lambda peer: route_ref, route_line, 6, route_sem)
    for index in (6, 7, 8, 3, 4, 5, 0, 1, 2):
        loads[index].start()

    loads[6].wait()
    loads[7].wait()
    input_pre = (
        across(normed, input_weight[...])
        + input_bias_ref[...]
    )
    forget_pre = (
        across(normed, forget_weight[...])
        + forget_bias_ref[...]
    )
    carried = (
        jnp.minimum(forget_pre, 0.0)
        - jnp.log1p(jnp.exp(-jnp.abs(forget_pre)))
        + stabilizer_ref[...]
    )
    next_stabilizer = jnp.maximum(carried, input_pre)
    keep_old = jnp.exp(carried - next_stabilizer)
    write_new = jnp.exp(input_pre - next_stabilizer)
    gates_ref[0] = keep_old
    gates_ref[1] = write_new
    next_stabilizer_ref[...] = next_stabilizer
    rounds, _, local, capacity, far = outgoing.shape
    width = tokens_ref.shape[1]
    near = width - far
    slot_count = n * local * capacity
    near_slots = members * local * capacity
    dispatch, combine = [], []
    for turn in range(rounds):
        slots, combined = routing(
            ids_ref[...], route_ref[...], 0, slot_count, capacity, turn * capacity
        )
        dispatch.append(slots.T.astype(jnp.bfloat16))
        combine.append(combined)
    sequences, heads, head_width = memory.shape[:3]
    loads[8].wait()

    def split(s, carry):
        for head in range(heads):
            value = memory[s, head]
            high = value.astype(jnp.bfloat16)
            rows = pl.ds(pl.multiple_of(s * head_width, LANES), head_width)
            split_buf[head, rows, :head_width] = high
            split_buf[head, rows, head_width:] = (value - high.astype(jnp.float32)).astype(
                jnp.bfloat16
            )
        return carry

    lax.fori_loop(0, sequences, split, 0)

    def exchange(source, target, arrival, order, corners=None):
        def one(group, member, peer):
            send(source.at[peer], target.at[me], send_sem, arrival, peer)

        each_peer(one, 1, order, corners)

    drain(rows_buf.at[:, core], recv_sems.at[0])
    send(
        rows_buf.at[:, core], rows_buf.at[:, core], send_sem, recv_sems.at[3], partner
    )
    for half in range(halves):
        drain(weight_buf.at[half], weight_sems.at[half])
        if half == 0:
            drain(rows_buf.at[:, 1 - core], recv_sems.at[3])
        rows = rows_buf[...].reshape(n * rows_buf.shape[2], part_width)
        weight = weight_buf[half].reshape(members * weight_buf.shape[2], half_columns)
        product = jnp.dot(rows, weight, preferred_element_type=jnp.float32)
        product_buf[half] = product.reshape(product_buf.shape[1:]).astype(jnp.bfloat16)
        pltpu.make_async_copy(
            product_buf.at[half, me], result_buf.at[half, me], result_sems.at[half]
        ).start()
        exchange(product_buf.at[half], result_buf.at[half], result_sems.at[half], DOWN)

    def send_mix(member):
        send(
            mix_ref,
            mix_buf.at[near_chip, core],
            send_sem,
            mix_sems.at[near_chip],
            plane * members + member,
        )

    each_near(send_mix, 2)

    def forward_mix(member):
        index = lax.div(member, 2)
        drain(mix_buf.at[index, core], mix_sems.at[index])
        send(
            mix_buf.at[index, core],
            mix_buf.at[index, core],
            send_sem,
            recv_sems.at[4],
            partner,
        )

    forward_mix(place)
    drain(ids_line, recv_sems.at[5])
    drain(route_line, recv_sems.at[6])
    for turn in range(rounds):
        for group in range(groups):
            near_chosen, near_combine = routing(
                ids_line[group],
                route_line[group],
                plane * near_slots,
                near_slots,
                capacity,
                turn * capacity,
            )
            dispatch_line[turn, group] = near_chosen.T.astype(jnp.bfloat16)
            near_high = near_combine.astype(jnp.bfloat16)
            combine_line[turn, group, :sequences] = near_high
            combine_line[turn, group, sequences:] = (
                near_combine - near_high.astype(jnp.float32)
            ).astype(jnp.bfloat16)
    memory_width = heads * head_width
    row = lax.broadcasted_iota(jnp.int32, (sequences, head_width), 0)

    def read_head(head):
        def piece(matrix):
            start = matrix * memory_width + head * head_width
            return projected_ref[:, start : start + head_width]

        span = slice(head * head_width, (head + 1) * head_width)
        query, value, out_gate = piece(0), piece(2), piece(3)
        key = piece(1) * head_width ** (-0.5)
        keep, write = keep_old[:, head : head + 1], write_new[:, head : head + 1]
        local_score = write * jnp.sum(query * key, axis=-1, keepdims=True)
        denominator = (
            keep * jnp.sum(normalizer_ref[:, head, :] * query, axis=-1, keepdims=True) + local_score
        )
        narrow = query.astype(jnp.bfloat16)
        reads = lax.dot_general(
            jnp.concatenate([narrow, narrow], axis=1),
            split_buf[head],
            (((1,), (1,)), ((), ())),
            preferred_element_type=jnp.float32,
        )
        read = jnp.zeros((sequences, head_width), jnp.float32)
        for s in range(sequences):
            read = jnp.where(row == s, reads[:, s * head_width : (s + 1) * head_width], read)
        memory_read = (keep * read + local_score * value) / jnp.maximum(
            jnp.abs(denominator), 1.0
        )
        gated_src[:, span] = (jax.nn.sigmoid(out_gate) * memory_read).astype(jnp.bfloat16)

    for half in range(halves):
        drain(result_buf.at[half], result_sems.at[half])
        for member in range(members):
            total = result_buf[half, member].astype(jnp.float32)
            for group in range(1, groups):
                total = total + result_buf[half, group * members + member].astype(jnp.float32)
            total = total.astype(jnp.bfloat16).astype(jnp.float32)
            start = member * columns + half * half_columns
            projected_ref[:, start : start + half_columns] = total
        for head in range(heads):
            if head * head_width % columns // half_columns == half:
                read_head(head)

    pltpu.make_async_copy(gated_src, gated_buf.at[plane], recv_sems.at[1]).start()
    line(lambda peer: gated_src, gated_buf, 1)
    key_scale = head_width ** (-0.5)
    for head in range(heads):
        start = memory_width + head * head_width
        next_normalizer_ref[:, head, :] = keep_old[:, head : head + 1] * normalizer_ref[
            :, head, :
        ] + write_new[:, head : head + 1] * (
            projected_ref[:, start : start + head_width] * key_scale
        )

    def update(s, carry):
        line_of = pl.ds(s, 1)
        keep, write = gates_ref[0, line_of, :], gates_ref[1, line_of, :]
        keys = projected_ref[line_of, memory_width : 2 * memory_width] * key_scale
        values = projected_ref[line_of, 2 * memory_width : 3 * memory_width]
        stacked = jnp.concatenate(
            [
                write[:, head : head + 1] * values[:, head * head_width : (head + 1) * head_width]
                for head in range(heads)
            ],
            axis=0,
        ).T
        for head in range(heads):
            next_memory_ref[s, head] = (
                keep[:, head : head + 1] * memory[s, head]
                + stacked[:, head : head + 1]
                * keys[:, head * head_width : (head + 1) * head_width]
            )
        return carry

    lax.fori_loop(0, sequences // 2, update, 0)
    around(range(2, CUBE, 2), forward_mix, False)
    drain(gated_buf, recv_sems.at[1])
    drain(mix_buf.at[:, 1 - core], recv_sems.at[4])
    gated = gated_buf[...].reshape(gated_buf.shape[0] * gated_buf.shape[1], gated_buf.shape[2])
    mix_weight = mix_buf[...].reshape(members * mix_buf.shape[2], mix_buf.shape[3])
    columns_buf[...] = (
        lax.dot_general(
            gated, mix_weight, (((1,), (1,)), ((), ())), preferred_element_type=jnp.float32
        )
        .reshape(columns_buf.shape)
        .astype(jnp.bfloat16)
    )
    pltpu.make_async_copy(columns_buf.at[plane], mixed_buf.at[plane], recv_sems.at[2]).start()
    line(lambda peer: columns_buf.at[peer], mixed_buf, 2)
    lax.fori_loop(sequences // 2, sequences, update, 0)
    drain(mixed_buf, recv_sems.at[2])
    mixed = jnp.concatenate([mixed_buf[group] for group in range(groups)], axis=1)
    after_mix = (residual + rms_scale(mixed.astype(jnp.float32), postmix_ref[...])).astype(
        jnp.bfloat16
    )
    after_float = after_mix.astype(jnp.float32)
    token_rows = rms_scale(after_float, prefeed_ref[...]).astype(jnp.bfloat16)
    line_rows[plane] = token_rows[:, far:]
    for mask in range(groups - 1, 0, -1):
        send(
            line_rows.at[plane],
            line_rows.at[plane],
            send_sem,
            line_sems.at[mask],
            flip(plane, mask) * members + place,
        )

    def deal(turn, group):
        near_out[turn, group] = (
            jnp.dot(
                dispatch_line[turn, group], line_rows[group], preferred_element_type=jnp.float32
            )
            .reshape(near_out.shape[2:])
            .astype(jnp.bfloat16)
        )
        pltpu.make_async_copy(
            near_out.at[turn, group, place], near_in.at[turn, group, place], near_sems.at[turn]
        ).start()

        def one(member):
            send(
                near_out.at[turn, group, member],
                near_in.at[turn, group, place],
                send_sem,
                near_sems.at[turn],
                plane * members + member,
            )

        each_near(one)

    def deal_far(turn):
        outgoing[turn] = (
            jnp.dot(dispatch[turn], token_rows[:, :far], preferred_element_type=jnp.float32)
            .reshape(outgoing.shape[1:])
            .astype(jnp.bfloat16)
        )
        pltpu.make_async_copy(
            outgoing.at[turn, me], arrived.at[turn, me], far_sems.at[turn]
        ).start()
        exchange(outgoing.at[turn], arrived.at[turn], far_sems.at[turn], UP, range(CUBE))

    deal(0, plane)
    deal_far(0)
    for turn in range(1, rounds):
        deal(turn, plane)
    for mask in range(1, groups):
        source = flip(plane, mask)
        drain(line_rows.at[source], line_sems.at[mask])
        deal(0, source)
    for turn in range(1, rounds):
        deal_far(turn)
        for mask in range(1, groups):
            deal(turn, flip(plane, mask))
    for index in (3, 4, 5):
        loads[index].wait()
    shared_out = two_layer(token_rows, weights[3][...], weights[4][...], weights[5][...])
    for index in (0, 1, 2):
        loads[index].wait()
    back = returned.shape[4]
    near = width - far

    def work(turn):
        drain(near_in.at[turn], near_sems.at[turn])
        drain(arrived.at[turn], far_sems.at[turn])
        inner_rows = []
        for item in range(local):
            block = jnp.concatenate(
                [
                    arrived[turn, :, item].astype(jnp.float32).reshape(slot_count // local, far),
                    near_in[turn, :, :, item]
                    .astype(jnp.float32)
                    .reshape(slot_count // local, near),
                ],
                axis=1,
            ).astype(jnp.bfloat16)
            inner = gated_rows(block, weights[0][item], weights[1][item])
            inner_rows.append(inner)
            near_answer[turn, :, :, item] = (
                jnp.dot(inner, weights[2][item, :, back:], preferred_element_type=jnp.float32)
                .reshape(groups, members, capacity, width - back)
                .astype(jnp.bfloat16)
            )
        pltpu.make_async_copy(
            near_answer.at[turn, :, place], near_back.at[turn, :, place], back_sems.at[turn]
        ).start()

        def one(member):
            send(
                near_answer.at[turn, :, member],
                near_back.at[turn, :, place],
                send_sem,
                back_sems.at[turn],
                plane * members + member,
            )

        each_near(one)
        return inner_rows

    def work_far(turn, inner_rows):
        for item in range(local):
            answer[turn, :, item] = (
                jnp.dot(
                    inner_rows[item], weights[2][item, :, :back], preferred_element_type=jnp.float32
                )
                .reshape(n, capacity, back)
                .astype(jnp.bfloat16)
            )
        pltpu.make_async_copy(
            answer.at[turn, me], returned.at[turn, me], home_sems.at[turn]
        ).start()
        exchange(answer.at[turn], returned.at[turn], home_sems.at[turn], DOWN, range(CUBE))

    def weigh(turn, group):
        rows = near_back[turn, group].astype(jnp.float32).reshape(near_slots, width - back)
        both = jnp.dot(
            combine_line[turn, group], rows.astype(jnp.bfloat16), preferred_element_type=jnp.float32
        )
        return both[:sequences] + both[sequences:]

    def far_part(turn):
        drain(returned.at[turn], home_sems.at[turn])
        picked = returned[turn].astype(jnp.float32).reshape(slot_count, back).astype(jnp.bfloat16)
        high = combine[turn].astype(jnp.bfloat16)
        low = (combine[turn] - high.astype(jnp.float32)).astype(jnp.bfloat16)
        return jnp.dot(high, picked, preferred_element_type=jnp.float32) + jnp.dot(
            low, picked, preferred_element_type=jnp.float32
        )

    for turn in range(rounds):
        work_far(turn, work(turn))
    last = rounds - 1
    far_sum = shared_out[:, :back]
    for turn in range(last):
        drain(near_back.at[turn], back_sems.at[turn])
        for i in range(groups):
            peer = flip(plane, i)
            known = weigh(turn, peer)
            near_sums[i] = known if turn == 0 else near_sums[i] + known
    drain(near_back.at[last], back_sems.at[last])
    for i in range(groups - 1, -1, -1):
        peer = flip(plane, i)
        total = weigh(last, peer)
        if last:
            total = total + near_sums[i]
        if i:
            partial_out[peer] = total.astype(jnp.bfloat16)
    for i in range(groups - 1, 0, -1):
        peer = flip(plane, i)
        send(
            partial_out.at[peer],
            partial_in.at[i],
            send_sem,
            recv_sems.at[7],
            peer * members + place,
        )
    near_sum = shared_out[:, back:] + total
    for turn in range(rounds):
        far_sum = far_sum + far_part(turn)
    drain(partial_in.at[pl.ds(1, groups - 1)], recv_sems.at[7])
    for i in range(1, groups):
        near_sum = near_sum + partial_in[i].astype(jnp.float32)
    combined = jnp.concatenate([far_sum, near_sum], axis=1)
    out_ref[...] = (after_float + rms_scale(combined, postfeed_ref[...])).astype(jnp.bfloat16)
    drain(sent, send_sem)
    drain(ids_line.at[pl.ds(0, groups - 1)], line_sems.at[0])
    drain(route_line.at[pl.ds(0, groups - 1)], route_sem)


def layer(n, groups, small, projections, loads, capacity):
    tokens, mix_weight = small[0], small[-1]
    sequences, width = tokens.shape
    depth, columns = projections[0].shape
    members = n // groups
    wide = 4 * columns // members
    halves = max(1, min(HALVES, wide // LANES))
    local = loads[0].shape[0]
    heads, head_width = loads[8].shape[1:3]
    narrow = functools.partial(pltpu.VMEM, dtype=jnp.bfloat16)
    far = width * FAR_IN // 8 // LANES * LANES
    back = width * FAR_OUT // 8 // LANES * LANES
    rounds = ROUNDS if capacity % (2 * ROUNDS) == 0 else 1
    capacity = capacity // rounds
    near_slots = members * local * capacity

    chips, near_chips = n // 2, members // 2
    slot_rows = rounds * local * capacity
    sent = (
        (2 * chips - 1) * sequences * (width // groups)
        + (members - 1) * depth * wide
        + (n - 1) * sequences * wide
        + (2 * near_chips - 1) * mix_weight.size
        + (groups - 1) * sequences * (columns + width // groups + 2 * width - far - back)
        + (n - 1) * slot_rows * (far + back)
        + groups * (members - 1) * slot_rows * (2 * width - far - back)
    )

    def slots(size):
        return [narrow((rounds, n, local, capacity, size))] * 2

    def blocks(size):
        return [narrow((rounds, groups, members, local, capacity, size))] * 2

    def rows(size):
        return [narrow((groups, sequences, size))]

    choices = small[9].shape[1]
    pieces = narrow((groups, sequences, width // groups))
    return pl.pallas_call(
        functools.partial(layer_kernel, n, groups),
        out_shape=(
            pltpu.VMEM((sequences, width), jnp.bfloat16),
            pltpu.VMEM(loads[8].shape, jnp.float32),
            pltpu.VMEM((sequences, heads, head_width), jnp.float32),
            pltpu.VMEM((sequences, heads), jnp.float32),
        ),
        in_specs=[ANY] * (len(small) + len(projections) + len(loads)),
        out_specs=(VM,) * 4,
        scratch_shapes=[pltpu.VMEM(w.shape, w.dtype) for w in small]
        + [narrow((len(projections), depth, columns))]
        + [pltpu.VMEM(w.shape, w.dtype) for w in loads]
        + [
            pieces,
            narrow((n // 2, 2, sequences, width // groups)),
            narrow((halves, members, depth, wide // halves)),
            narrow((halves, n, sequences, wide // halves)),
            narrow((halves, n, sequences, wide // halves)),
            narrow((members // 2, 2) + mix_weight.shape),
            narrow((heads, sequences * head_width, 2 * head_width)),
            narrow((sequences, columns)),
            narrow((groups, sequences, columns)),
            pieces,
            pieces,
        ]
        + slots(far)
        + slots(back)
        + rows(width - far)
        + blocks(width - far)
        + blocks(width - back)
        + rows(width - back) * 2
        + [
            pltpu.VMEM((groups, sequences, choices), jnp.int32),
            pltpu.VMEM((groups, sequences, choices), jnp.float32),
            narrow((rounds, groups, near_slots, sequences)),
            narrow((rounds, groups, 2 * sequences, near_slots)),
            pltpu.VMEM((groups, sequences, width - back), jnp.float32),
            pltpu.VMEM((sequences, 4 * columns), jnp.float32),
            pltpu.VMEM((2, sequences, heads), jnp.float32),
            narrow((sent // LANES, LANES)),
            pltpu.SemaphoreType.DMA((len(small),)),
            pltpu.SemaphoreType.DMA,
            pltpu.SemaphoreType.DMA((len(loads),)),
            pltpu.SemaphoreType.DMA,
            pltpu.SemaphoreType.DMA,
            pltpu.SemaphoreType.DMA((8,)),
            pltpu.SemaphoreType.DMA((groups,)),
            pltpu.SemaphoreType.DMA((halves,)),
            pltpu.SemaphoreType.DMA((halves,)),
            pltpu.SemaphoreType.DMA((members // 2,)),
            pltpu.SemaphoreType.DMA((rounds,)),
            pltpu.SemaphoreType.DMA((rounds,)),
            pltpu.SemaphoreType.DMA((rounds,)),
            pltpu.SemaphoreType.DMA((rounds,)),
        ],
        compiler_params=pltpu.CompilerParams(
            collective_id=0, has_side_effects=True, vmem_limit_bytes=54 * 1024 * 1024
        ),
    )(
        *[
            pltpu.with_memory_space_constraint(w, pltpu.HBM)
            for w in small + projections + loads
        ],
    )


def publish_kernel(*refs):
    count = len(refs) // 2
    sems = refs[-1]
    copies = [
        pltpu.make_async_copy(refs[index], refs[count + index], sems.at[index])
        for index in range(count)
    ]
    for copy in copies:
        copy.start()
    for copy in copies:
        copy.wait()


def publish(*results):
    held = [pltpu.with_memory_space_constraint(result, pltpu.VMEM) for result in results]
    return pl.pallas_call(
        publish_kernel,
        out_shape=tuple(jax.ShapeDtypeStruct(r.shape, r.dtype) for r in results),
        in_specs=[VM] * len(results),
        out_specs=(ANY,) * len(results),
        scratch_shapes=[pltpu.SemaphoreType.DMA((len(results),))],
        compiler_params=pltpu.CompilerParams(vmem_limit_bytes=1024 * 1024),
    )(*held)


def on_device(
    tokens,
    premix_gain,
    postmix_gain,
    prefeed_gain,
    postfeed_gain,
    query_weight,
    key_weight,
    value_weight,
    outgate_weight,
    ingate_weight,
    forget_weight,
    ingate_bias,
    forget_bias,
    memory_state,
    normalizer,
    stabilizer,
    output_weight,
    expert_ids,
    route_weights,
    expert_gate,
    expert_up,
    expert_down,
    shared_gate,
    shared_up,
    shared_down,
):
    sequences = tokens.shape[0]
    devices = lax.axis_size("ep")
    experts_total = expert_gate.shape[0] * devices
    choose_count = expert_ids.shape[1]
    capacity = min(
        sequences, max(2, 2 * ((sequences * choose_count + experts_total - 1) // experts_total))
    )
    results = layer(
        devices,
        GROUPS,
        (
            tokens,
            premix_gain[None],
            postmix_gain[None],
            prefeed_gain[None],
            postfeed_gain[None],
            ingate_bias[None],
            forget_bias[None],
            normalizer,
            stabilizer,
            expert_ids,
            route_weights,
            output_weight.T,
        ),
        (query_weight, key_weight, value_weight, outgate_weight),
        (
            expert_gate,
            expert_up,
            expert_down,
            shared_gate,
            shared_up,
            shared_down,
            ingate_weight.T,
            forget_weight.T,
            memory_state,
        ),
        capacity,
    )
    return publish(*results)


def solution(mesh):
    in_specs = (
        P("ep", None),
        P(),
        P(),
        P(),
        P(),
        P("ep", None),
        P("ep", None),
        P("ep", None),
        P("ep", None),
        P(),
        P(),
        P(),
        P(),
        P("ep", None, None, None),
        P("ep", None, None),
        P("ep", None),
        P(None, "ep"),
        P("ep", None),
        P("ep", None),
        P("ep", None, None),
        P("ep", None, None),
        P("ep", None, None),
        P(),
        P(),
        P(),
    )
    out_specs = (P("ep", None), P("ep", None, None, None), P("ep", None, None), P("ep", None))
    return jax.shard_map(
        on_device, mesh=mesh, in_specs=in_specs, out_specs=out_specs, check_vma=False
    )
```

```python
import functools

import jax
import jax.numpy as jnp
from jax import lax
from jax.experimental import pallas as pl
from jax.experimental.pallas import tpu as pltpu
from jax.sharding import PartitionSpec as P

epsilon = 1e-06
LANES = 128
GROUPS = 4
FAR_IN = 4
FAR_OUT = 4
ROUNDS = 2
CUBE = 8
HALVES = 4
MESH = pl.DeviceIdType.MESH
VM = pl.BlockSpec(memory_space=pltpu.VMEM)
ANY = pl.BlockSpec(memory_space=pl.ANY)


def rms_scale(values, gain_row):
    return (
        values * lax.rsqrt(jnp.mean(values * values, axis=-1, keepdims=True) + epsilon) * gain_row
    )


def greet(n, me):
    sem = pltpu.get_barrier_semaphore()

    def signal(i, carry):
        pl.semaphore_signal(
            sem, inc=1, device_id=(lax.rem(me + i, n),), device_id_type=MESH
        )
        return carry

    lax.fori_loop(1, n, signal, 0)


def greeted(n):
    pl.semaphore_wait(pltpu.get_barrier_semaphore(), n - 1)


def send(src, dst, send_sem, recv_sem, peer):
    pltpu.make_async_remote_copy(
        src_ref=src,
        dst_ref=dst,
        send_sem=send_sem,
        recv_sem=recv_sem,
        device_id=(peer,),
        device_id_type=MESH,
    ).start()


def drain(ref, sem):
    pltpu.make_async_copy(ref, ref, sem).wait()


def flip(value, mask):
    result, bit = value, 1
    while bit <= mask:
        if mask & bit:
            result = result + bit * (1 - 2 * lax.rem(lax.div(value, bit), 2))
        bit *= 2
    return result


def routing(ids, route_weights, first_slot, slot_count, capacity, first_turn):
    sequences, choices = ids.shape
    slot = (
        first_slot + lax.broadcasted_iota(jnp.int32, (sequences, slot_count), 1)
    ).astype(jnp.float32)
    owner = jnp.floor((slot + 0.5) * (1.0 / capacity))
    turn = slot - owner * capacity + first_turn
    chosen = jnp.zeros((sequences, slot_count), jnp.float32)
    weight_of = jnp.zeros((sequences, slot_count), jnp.float32)
    float_ids = ids.astype(jnp.float32)
    for choice in range(choices):
        same = float_ids[:, choice : choice + 1] == owner
        chosen = jnp.where(same, 1.0, chosen)
        weight_of = jnp.where(same, route_weights[:, choice : choice + 1], weight_of)
    earlier = jnp.zeros((sequences, slot_count), jnp.float32)
    row = lax.broadcasted_iota(jnp.int32, (sequences, slot_count), 0)
    for other in range(sequences - 1):
        earlier = earlier + jnp.where(row > other, chosen[other : other + 1], 0.0)
    slots = jnp.where(earlier == turn, chosen, 0.0)
    return slots, slots * weight_of


def across(left, right):
    return lax.dot_general(
        left, right, (((1,), (1,)), ((), ())), preferred_element_type=jnp.float32
    )


def gated_rows(rows, gate_weight, up_weight):
    gate_values = jnp.dot(rows, gate_weight, preferred_element_type=jnp.float32)
    up_values = jnp.dot(rows, up_weight, preferred_element_type=jnp.float32)
    return (gate_values * jax.nn.sigmoid(gate_values) * up_values).astype(jnp.bfloat16)


def two_layer(rows, gate_weight, up_weight, down_weight):
    inner_rows = gated_rows(rows, gate_weight, up_weight)
    return jnp.dot(inner_rows, down_weight, preferred_element_type=jnp.float32)


def layer_kernel(n, groups, *refs):
    small_from = refs[:12]
    projections = refs[12:16]
    loads_from = refs[16:25]
    out_ref, next_memory_ref, next_normalizer_ref, next_stabilizer_ref = refs[25:29]
    small = refs[29:41]
    (
        tokens_ref,
        premix_ref,
        postmix_ref,
        prefeed_ref,
        postfeed_ref,
        input_bias_ref,
        forget_bias_ref,
        normalizer_ref,
        stabilizer_ref,
        ids_ref,
        route_ref,
        mix_ref,
    ) = small
    staged = refs[41]
    loaded = refs[42:51]
    (
        normed_buf,
        rows_buf,
        weight_buf,
        product_buf,
        result_buf,
        mix_buf,
        split_buf,
        gated_src,
        gated_buf,
        columns_buf,
        mixed_buf,
        outgoing,
        arrived,
        answer,
        returned,
        line_rows,
        near_out,
        near_in,
        near_answer,
        near_back,
        partial_out,
        partial_in,
        ids_line,
        route_line,
        dispatch_line,
        combine_line,
        near_sums,
        projected_ref,
        gates_ref,
        sent,
        small_sems,
        staged_sem,
        load_sems,
        send_sem,
        route_sem,
        recv_sems,
        line_sems,
        weight_sems,
        result_sems,
        mix_sems,
        near_sems,
        far_sems,
        back_sems,
        home_sems,
    ) = refs[51:]
    weights = loaded[:6]
    input_weight, forget_weight, memory = loaded[6:]
    me = lax.axis_index("ep")
    members = n // groups
    plane, place = me // members, lax.rem(me, members)
    chips, near_chips = n // 2, members // 2
    chip, core, near_chip = me // 2, lax.rem(me, 2), place // 2
    partner = me + 1 - 2 * core
    part_width = rows_buf.shape[3]
    halves, half_columns = weight_buf.shape[0], weight_buf.shape[3]
    columns = halves * half_columns
    per_matrix = staged.shape[2] // columns
    greet(n, me)
    small_loads = [
        pltpu.make_async_copy(source, target, small_sems.at[index])
        for index, (source, target) in enumerate(zip(small_from, small))
    ]
    staged_loads = [
        pltpu.make_async_copy(source, staged.at[index], staged_sem)
        for index, source in enumerate(projections)
    ]
    for copy in small_loads[:2] + staged_loads + small_loads[2:]:
        copy.start()
    cubes = members // CUBE
    UP, DOWN = range(groups), range(groups - 1, -1, -1)
    cube, corner = lax.div(place, CUBE), lax.rem(place, CUBE)

    def around(masks, body, include_own):
        def one(i, carry):
            base = lax.rem(cube + i, cubes) * CUBE
            for mask in masks:
                body(base + flip(corner, mask))
            return carry

        if not include_own:
            for mask in masks:
                if mask:
                    body(cube * CUBE + flip(corner, mask))
        lax.fori_loop(0 if include_own else 1, cubes, one, 0)

    def each_near(body, step=1):
        around(range(CUBE - step, -1, -step), body, False)

    def each_peer(body, step=1, order=range(groups - 1, -1, -1), corners=None):
        for mask in order:
            peers = flip(plane, mask)
            around(
                corners or range(CUBE - step, -1, -step),
                lambda member: body(peers, member, peers * members + member),
                mask > 0,
            )
    def column(block, half):
        start = lax.rem(block, per_matrix) * columns + half * half_columns
        return pl.ds(pl.multiple_of(start, LANES), half_columns)

    loads = [
        pltpu.make_async_copy(source, target, load_sems.at[index])
        for index, (source, target) in enumerate(zip(loads_from, loaded))
    ]
    for copy in small_loads[:2]:
        copy.wait()
    residual = tokens_ref[...].astype(jnp.float32)
    normed = rms_scale(residual, premix_ref[...]).astype(jnp.bfloat16)
    for group in range(groups):
        normed_buf[group] = normed[:, group * part_width : (group + 1) * part_width]
    pltpu.make_async_copy(
        normed_buf.at[plane], rows_buf.at[chip, core], recv_sems.at[0]
    ).start()
    drain(staged, staged_sem)
    for copy in small_loads[2:]:
        copy.wait()
    greeted(n)

    def send_rows(group, member, peer):
        send(
            normed_buf.at[group],
            rows_buf.at[chip, core],
            send_sem,
            recv_sems.at[0],
            peer,
        )

    def line(source, target, stage, leave=None):
        for mask in range(groups - 1, 0, -1):
            peer = flip(plane, mask)
            send(
                source(peer),
                target.at[plane],
                send_sem if leave is None else leave,
                recv_sems.at[stage],
                peer * members + place,
            )

    def send_weights(half):
        def one(block):
            send(
                staged.at[lax.div(block, per_matrix), :, column(block, half)],
                weight_buf.at[half, place],
                send_sem,
                weight_sems.at[half],
                plane * members + block,
            )

        each_near(one)

    each_peer(send_rows, 2)
    for half in range(halves):
        send_weights(half)
    for half in range(halves):
        pltpu.make_async_copy(
            staged.at[lax.div(place, per_matrix), :, column(place, half)],
            weight_buf.at[half, place],
            weight_sems.at[half],
        ).start()
    pltpu.make_async_copy(mix_ref, mix_buf.at[near_chip, core], mix_sems.at[near_chip]).start()
    pltpu.make_async_copy(ids_ref, ids_line.at[plane], recv_sems.at[5]).start()
    pltpu.make_async_copy(route_ref, route_line.at[plane], recv_sems.at[6]).start()
    line(lambda peer: ids_ref, ids_line, 5, line_sems.at[0])
    line(lambda peer: route_ref, route_line, 6, route_sem)
    for index in (6, 7, 8, 3, 4, 5, 0, 1, 2):
        loads[index].start()

    loads[6].wait()
    loads[7].wait()
    input_pre = (
        across(normed, input_weight[...])
        + input_bias_ref[...]
    )
    forget_pre = (
        across(normed, forget_weight[...])
        + forget_bias_ref[...]
    )
    carried = (
        jnp.minimum(forget_pre, 0.0)
        - jnp.log1p(jnp.exp(-jnp.abs(forget_pre)))
        + stabilizer_ref[...]
    )
    next_stabilizer = jnp.maximum(carried, input_pre)
    keep_old = jnp.exp(carried - next_stabilizer)
    write_new = jnp.exp(input_pre - next_stabilizer)
    gates_ref[0] = keep_old
    gates_ref[1] = write_new
    next_stabilizer_ref[...] = next_stabilizer
    rounds, _, local, capacity, far = outgoing.shape
    width = tokens_ref.shape[1]
    near = width - far
    slot_count = n * local * capacity
    near_slots = members * local * capacity
    dispatch, combine = [], []
    for turn in range(rounds):
        slots, combined = routing(
            ids_ref[...], route_ref[...], 0, slot_count, capacity, turn * capacity
        )
        dispatch.append(slots.T.astype(jnp.bfloat16))
        combine.append(combined)
    sequences, heads, head_width = memory.shape[:3]
    loads[8].wait()

    def split(s, carry):
        for head in range(heads):
            value = memory[s, head]
            high = value.astype(jnp.bfloat16)
            rows = pl.ds(pl.multiple_of(s * head_width, LANES), head_width)
            split_buf[head, rows, :head_width] = high
            split_buf[head, rows, head_width:] = (value - high.astype(jnp.float32)).astype(
                jnp.bfloat16
            )
        return carry

    lax.fori_loop(0, sequences, split, 0)

    def exchange(source, target, arrival, order, corners=None):
        def one(group, member, peer):
            send(source.at[peer], target.at[me], send_sem, arrival, peer)

        each_peer(one, 1, order, corners)

    drain(rows_buf.at[:, core], recv_sems.at[0])
    send(
        rows_buf.at[:, core], rows_buf.at[:, core], send_sem, recv_sems.at[3], partner
    )
    for half in range(halves):
        drain(weight_buf.at[half], weight_sems.at[half])
        if half == 0:
            drain(rows_buf.at[:, 1 - core], recv_sems.at[3])
        rows = rows_buf[...].reshape(n * rows_buf.shape[2], part_width)
        weight = weight_buf[half].reshape(members * weight_buf.shape[2], half_columns)
        product = jnp.dot(rows, weight, preferred_element_type=jnp.float32)
        product_buf[half] = product.reshape(product_buf.shape[1:]).astype(jnp.bfloat16)
        pltpu.make_async_copy(
            product_buf.at[half, me], result_buf.at[half, me], result_sems.at[half]
        ).start()
        exchange(product_buf.at[half], result_buf.at[half], result_sems.at[half], DOWN)

    def send_mix(member):
        send(
            mix_ref,
            mix_buf.at[near_chip, core],
            send_sem,
            mix_sems.at[near_chip],
            plane * members + member,
        )

    each_near(send_mix, 2)

    def forward_mix(member):
        index = lax.div(member, 2)
        drain(mix_buf.at[index, core], mix_sems.at[index])
        send(
            mix_buf.at[index, core],
            mix_buf.at[index, core],
            send_sem,
            recv_sems.at[4],
            partner,
        )

    forward_mix(place)
    drain(ids_line, recv_sems.at[5])
    drain(route_line, recv_sems.at[6])
    for turn in range(rounds):
        for group in range(groups):
            near_chosen, near_combine = routing(
                ids_line[group],
                route_line[group],
                plane * near_slots,
                near_slots,
                capacity,
                turn * capacity,
            )
            dispatch_line[turn, group] = near_chosen.T.astype(jnp.bfloat16)
            near_high = near_combine.astype(jnp.bfloat16)
            combine_line[turn, group, :sequences] = near_high
            combine_line[turn, group, sequences:] = (
                near_combine - near_high.astype(jnp.float32)
            ).astype(jnp.bfloat16)
    memory_width = heads * head_width
    row = lax.broadcasted_iota(jnp.int32, (sequences, head_width), 0)

    def read_head(head):
        def piece(matrix):
            start = matrix * memory_width + head * head_width
            return projected_ref[:, start : start + head_width]

        span = slice(head * head_width, (head + 1) * head_width)
        query, value, out_gate = piece(0), piece(2), piece(3)
        key = piece(1) * head_width ** (-0.5)
        keep, write = keep_old[:, head : head + 1], write_new[:, head : head + 1]
        local_score = write * jnp.sum(query * key, axis=-1, keepdims=True)
        denominator = (
            keep * jnp.sum(normalizer_ref[:, head, :] * query, axis=-1, keepdims=True) + local_score
        )
        narrow = query.astype(jnp.bfloat16)
        reads = lax.dot_general(
            jnp.concatenate([narrow, narrow], axis=1),
            split_buf[head],
            (((1,), (1,)), ((), ())),
            preferred_element_type=jnp.float32,
        )
        read = jnp.zeros((sequences, head_width), jnp.float32)
        for s in range(sequences):
            read = jnp.where(row == s, reads[:, s * head_width : (s + 1) * head_width], read)
        memory_read = (keep * read + local_score * value) / jnp.maximum(
            jnp.abs(denominator), 1.0
        )
        gated_src[:, span] = (jax.nn.sigmoid(out_gate) * memory_read).astype(jnp.bfloat16)

    for half in range(halves):
        drain(result_buf.at[half], result_sems.at[half])
        for member in range(members):
            total = result_buf[half, member].astype(jnp.float32)
            for group in range(1, groups):
                total = total + result_buf[half, group * members + member].astype(jnp.float32)
            total = total.astype(jnp.bfloat16).astype(jnp.float32)
            start = member * columns + half * half_columns
            projected_ref[:, start : start + half_columns] = total
        for head in range(heads):
            if head * head_width % columns // half_columns == half:
                read_head(head)

    pltpu.make_async_copy(gated_src, gated_buf.at[plane], recv_sems.at[1]).start()
    line(lambda peer: gated_src, gated_buf, 1)
    key_scale = head_width ** (-0.5)
    for head in range(heads):
        start = memory_width + head * head_width
        next_normalizer_ref[:, head, :] = keep_old[:, head : head + 1] * normalizer_ref[
            :, head, :
        ] + write_new[:, head : head + 1] * (
            projected_ref[:, start : start + head_width] * key_scale
        )

    def update(s, carry):
        line_of = pl.ds(s, 1)
        keep, write = gates_ref[0, line_of, :], gates_ref[1, line_of, :]
        keys = projected_ref[line_of, memory_width : 2 * memory_width] * key_scale
        values = projected_ref[line_of, 2 * memory_width : 3 * memory_width]
        stacked = jnp.concatenate(
            [
                write[:, head : head + 1] * values[:, head * head_width : (head + 1) * head_width]
                for head in range(heads)
            ],
            axis=0,
        ).T
        for head in range(heads):
            next_memory_ref[s, head] = (
                keep[:, head : head + 1] * memory[s, head]
                + stacked[:, head : head + 1]
                * keys[:, head * head_width : (head + 1) * head_width]
            )
        return carry

    lax.fori_loop(0, sequences // 4, update, 0)
    around(range(2, CUBE, 2), forward_mix, False)
    drain(gated_buf, recv_sems.at[1])
    drain(mix_buf.at[:, 1 - core], recv_sems.at[4])
    gated = gated_buf[...].reshape(gated_buf.shape[0] * gated_buf.shape[1], gated_buf.shape[2])
    mix_weight = mix_buf[...].reshape(members * mix_buf.shape[2], mix_buf.shape[3])
    columns_buf[...] = (
        lax.dot_general(
            gated, mix_weight, (((1,), (1,)), ((), ())), preferred_element_type=jnp.float32
        )
        .reshape(columns_buf.shape)
        .astype(jnp.bfloat16)
    )
    pltpu.make_async_copy(columns_buf.at[plane], mixed_buf.at[plane], recv_sems.at[2]).start()
    line(lambda peer: columns_buf.at[peer], mixed_buf, 2)
    lax.fori_loop(sequences // 4, sequences, update, 0)
    drain(mixed_buf, recv_sems.at[2])
    mixed = jnp.concatenate([mixed_buf[group] for group in range(groups)], axis=1)
    after_mix = (residual + rms_scale(mixed.astype(jnp.float32), postmix_ref[...])).astype(
        jnp.bfloat16
    )
    after_float = after_mix.astype(jnp.float32)
    token_rows = rms_scale(after_float, prefeed_ref[...]).astype(jnp.bfloat16)
    line_rows[plane] = token_rows[:, far:]
    for mask in range(groups - 1, 0, -1):
        send(
            line_rows.at[plane],
            line_rows.at[plane],
            send_sem,
            line_sems.at[mask],
            flip(plane, mask) * members + place,
        )

    def deal(turn, group):
        near_out[turn, group] = (
            jnp.dot(
                dispatch_line[turn, group], line_rows[group], preferred_element_type=jnp.float32
            )
            .reshape(near_out.shape[2:])
            .astype(jnp.bfloat16)
        )
        pltpu.make_async_copy(
            near_out.at[turn, group, place], near_in.at[turn, group, place], near_sems.at[turn]
        ).start()

        def one(member):
            send(
                near_out.at[turn, group, member],
                near_in.at[turn, group, place],
                send_sem,
                near_sems.at[turn],
                plane * members + member,
            )

        each_near(one)

    def deal_far(turn):
        outgoing[turn] = (
            jnp.dot(dispatch[turn], token_rows[:, :far], preferred_element_type=jnp.float32)
            .reshape(outgoing.shape[1:])
            .astype(jnp.bfloat16)
        )
        pltpu.make_async_copy(
            outgoing.at[turn, me], arrived.at[turn, me], far_sems.at[turn]
        ).start()
        exchange(outgoing.at[turn], arrived.at[turn], far_sems.at[turn], UP, range(CUBE))

    deal(0, plane)
    deal_far(0)
    for turn in range(1, rounds):
        deal(turn, plane)
    for mask in range(1, groups):
        source = flip(plane, mask)
        drain(line_rows.at[source], line_sems.at[mask])
        deal(0, source)
    for turn in range(1, rounds):
        deal_far(turn)
        for mask in range(1, groups):
            deal(turn, flip(plane, mask))
    for index in (3, 4, 5):
        loads[index].wait()
    shared_out = two_layer(token_rows, weights[3][...], weights[4][...], weights[5][...])
    for index in (0, 1, 2):
        loads[index].wait()
    back = returned.shape[4]
    near = width - far

    def work(turn):
        drain(near_in.at[turn], near_sems.at[turn])
        drain(arrived.at[turn], far_sems.at[turn])
        inner_rows = []
        for item in range(local):
            block = jnp.concatenate(
                [
                    arrived[turn, :, item].astype(jnp.float32).reshape(slot_count // local, far),
                    near_in[turn, :, :, item]
                    .astype(jnp.float32)
                    .reshape(slot_count // local, near),
                ],
                axis=1,
            ).astype(jnp.bfloat16)
            inner = gated_rows(block, weights[0][item], weights[1][item])
            inner_rows.append(inner)
            near_answer[turn, :, :, item] = (
                jnp.dot(inner, weights[2][item, :, back:], preferred_element_type=jnp.float32)
                .reshape(groups, members, capacity, width - back)
                .astype(jnp.bfloat16)
            )
        pltpu.make_async_copy(
            near_answer.at[turn, :, place], near_back.at[turn, :, place], back_sems.at[turn]
        ).start()

        def one(member):
            send(
                near_answer.at[turn, :, member],
                near_back.at[turn, :, place],
                send_sem,
                back_sems.at[turn],
                plane * members + member,
            )

        each_near(one)
        return inner_rows

    def work_far(turn, inner_rows):
        for item in range(local):
            answer[turn, :, item] = (
                jnp.dot(
                    inner_rows[item], weights[2][item, :, :back], preferred_element_type=jnp.float32
                )
                .reshape(n, capacity, back)
                .astype(jnp.bfloat16)
            )
        pltpu.make_async_copy(
            answer.at[turn, me], returned.at[turn, me], home_sems.at[turn]
        ).start()
        exchange(answer.at[turn], returned.at[turn], home_sems.at[turn], DOWN, range(CUBE))

    def weigh(turn, group):
        rows = near_back[turn, group].astype(jnp.float32).reshape(near_slots, width - back)
        both = jnp.dot(
            combine_line[turn, group], rows.astype(jnp.bfloat16), preferred_element_type=jnp.float32
        )
        return both[:sequences] + both[sequences:]

    def far_part(turn):
        drain(returned.at[turn], home_sems.at[turn])
        picked = returned[turn].astype(jnp.float32).reshape(slot_count, back).astype(jnp.bfloat16)
        high = combine[turn].astype(jnp.bfloat16)
        low = (combine[turn] - high.astype(jnp.float32)).astype(jnp.bfloat16)
        return jnp.dot(high, picked, preferred_element_type=jnp.float32) + jnp.dot(
            low, picked, preferred_element_type=jnp.float32
        )

    for turn in range(rounds):
        work_far(turn, work(turn))
    last = rounds - 1
    far_sum = shared_out[:, :back]
    for turn in range(last):
        drain(near_back.at[turn], back_sems.at[turn])
        for i in range(groups):
            peer = flip(plane, i)
            known = weigh(turn, peer)
            near_sums[i] = known if turn == 0 else near_sums[i] + known
    drain(near_back.at[last], back_sems.at[last])
    for i in range(groups - 1, -1, -1):
        peer = flip(plane, i)
        total = weigh(last, peer)
        if last:
            total = total + near_sums[i]
        if i:
            partial_out[peer] = total.astype(jnp.bfloat16)
    for i in range(groups - 1, 0, -1):
        peer = flip(plane, i)
        send(
            partial_out.at[peer],
            partial_in.at[i],
            send_sem,
            recv_sems.at[7],
            peer * members + place,
        )
    near_sum = shared_out[:, back:] + total
    for turn in range(rounds):
        far_sum = far_sum + far_part(turn)
    drain(partial_in.at[pl.ds(1, groups - 1)], recv_sems.at[7])
    for i in range(1, groups):
        near_sum = near_sum + partial_in[i].astype(jnp.float32)
    combined = jnp.concatenate([far_sum, near_sum], axis=1)
    out_ref[...] = (after_float + rms_scale(combined, postfeed_ref[...])).astype(jnp.bfloat16)
    drain(sent, send_sem)
    drain(ids_line.at[pl.ds(0, groups - 1)], line_sems.at[0])
    drain(route_line.at[pl.ds(0, groups - 1)], route_sem)


def layer(n, groups, small, projections, loads, capacity):
    tokens, mix_weight = small[0], small[-1]
    sequences, width = tokens.shape
    depth, columns = projections[0].shape
    members = n // groups
    wide = 4 * columns // members
    halves = max(1, min(HALVES, wide // LANES))
    local = loads[0].shape[0]
    heads, head_width = loads[8].shape[1:3]
    narrow = functools.partial(pltpu.VMEM, dtype=jnp.bfloat16)
    far = width * FAR_IN // 8 // LANES * LANES
    back = width * FAR_OUT // 8 // LANES * LANES
    rounds = ROUNDS if capacity % (2 * ROUNDS) == 0 else 1
    capacity = capacity // rounds
    near_slots = members * local * capacity

    chips, near_chips = n // 2, members // 2
    slot_rows = rounds * local * capacity
    sent = (
        (2 * chips - 1) * sequences * (width // groups)
        + (members - 1) * depth * wide
        + (n - 1) * sequences * wide
        + (2 * near_chips - 1) * mix_weight.size
        + (groups - 1) * sequences * (columns + width // groups + 2 * width - far - back)
        + (n - 1) * slot_rows * (far + back)
        + groups * (members - 1) * slot_rows * (2 * width - far - back)
    )

    def slots(size):
        return [narrow((rounds, n, local, capacity, size))] * 2

    def blocks(size):
        return [narrow((rounds, groups, members, local, capacity, size))] * 2

    def rows(size):
        return [narrow((groups, sequences, size))]

    choices = small[9].shape[1]
    pieces = narrow((groups, sequences, width // groups))
    return pl.pallas_call(
        functools.partial(layer_kernel, n, groups),
        out_shape=(
            pltpu.VMEM((sequences, width), jnp.bfloat16),
            pltpu.VMEM(loads[8].shape, jnp.float32),
            pltpu.VMEM((sequences, heads, head_width), jnp.float32),
            pltpu.VMEM((sequences, heads), jnp.float32),
        ),
        in_specs=[ANY] * (len(small) + len(projections) + len(loads)),
        out_specs=(VM,) * 4,
        scratch_shapes=[pltpu.VMEM(w.shape, w.dtype) for w in small]
        + [narrow((len(projections), depth, columns))]
        + [pltpu.VMEM(w.shape, w.dtype) for w in loads]
        + [
            pieces,
            narrow((n // 2, 2, sequences, width // groups)),
            narrow((halves, members, depth, wide // halves)),
            narrow((halves, n, sequences, wide // halves)),
            narrow((halves, n, sequences, wide // halves)),
            narrow((members // 2, 2) + mix_weight.shape),
            narrow((heads, sequences * head_width, 2 * head_width)),
            narrow((sequences, columns)),
            narrow((groups, sequences, columns)),
            pieces,
            pieces,
        ]
        + slots(far)
        + slots(back)
        + rows(width - far)
        + blocks(width - far)
        + blocks(width - back)
        + rows(width - back) * 2
        + [
            pltpu.VMEM((groups, sequences, choices), jnp.int32),
            pltpu.VMEM((groups, sequences, choices), jnp.float32),
            narrow((rounds, groups, near_slots, sequences)),
            narrow((rounds, groups, 2 * sequences, near_slots)),
            pltpu.VMEM((groups, sequences, width - back), jnp.float32),
            pltpu.VMEM((sequences, 4 * columns), jnp.float32),
            pltpu.VMEM((2, sequences, heads), jnp.float32),
            narrow((sent // LANES, LANES)),
            pltpu.SemaphoreType.DMA((len(small),)),
            pltpu.SemaphoreType.DMA,
            pltpu.SemaphoreType.DMA((len(loads),)),
            pltpu.SemaphoreType.DMA,
            pltpu.SemaphoreType.DMA,
            pltpu.SemaphoreType.DMA((8,)),
            pltpu.SemaphoreType.DMA((groups,)),
            pltpu.SemaphoreType.DMA((halves,)),
            pltpu.SemaphoreType.DMA((halves,)),
            pltpu.SemaphoreType.DMA((members // 2,)),
            pltpu.SemaphoreType.DMA((rounds,)),
            pltpu.SemaphoreType.DMA((rounds,)),
            pltpu.SemaphoreType.DMA((rounds,)),
            pltpu.SemaphoreType.DMA((rounds,)),
        ],
        compiler_params=pltpu.CompilerParams(
            collective_id=0, has_side_effects=True, vmem_limit_bytes=54 * 1024 * 1024
        ),
    )(
        *[
            pltpu.with_memory_space_constraint(w, pltpu.HBM)
            for w in small + projections + loads
        ],
    )


def publish_kernel(*refs):
    count = len(refs) // 2
    sems = refs[-1]
    copies = [
        pltpu.make_async_copy(refs[index], refs[count + index], sems.at[index])
        for index in range(count)
    ]
    for copy in copies:
        copy.start()
    for copy in copies:
        copy.wait()


def publish(*results):
    held = [pltpu.with_memory_space_constraint(result, pltpu.VMEM) for result in results]
    return pl.pallas_call(
        publish_kernel,
        out_shape=tuple(jax.ShapeDtypeStruct(r.shape, r.dtype) for r in results),
        in_specs=[VM] * len(results),
        out_specs=(ANY,) * len(results),
        scratch_shapes=[pltpu.SemaphoreType.DMA((len(results),))],
        compiler_params=pltpu.CompilerParams(vmem_limit_bytes=1024 * 1024),
    )(*held)


def on_device(
    tokens,
    premix_gain,
    postmix_gain,
    prefeed_gain,
    postfeed_gain,
    query_weight,
    key_weight,
    value_weight,
    outgate_weight,
    ingate_weight,
    forget_weight,
    ingate_bias,
    forget_bias,
    memory_state,
    normalizer,
    stabilizer,
    output_weight,
    expert_ids,
    route_weights,
    expert_gate,
    expert_up,
    expert_down,
    shared_gate,
    shared_up,
    shared_down,
):
    sequences = tokens.shape[0]
    devices = lax.axis_size("ep")
    experts_total = expert_gate.shape[0] * devices
    choose_count = expert_ids.shape[1]
    capacity = min(
        sequences, max(2, 2 * ((sequences * choose_count + experts_total - 1) // experts_total))
    )
    results = layer(
        devices,
        GROUPS,
        (
            tokens,
            premix_gain[None],
            postmix_gain[None],
            prefeed_gain[None],
            postfeed_gain[None],
            ingate_bias[None],
            forget_bias[None],
            normalizer,
            stabilizer,
            expert_ids,
            route_weights,
            output_weight.T,
        ),
        (query_weight, key_weight, value_weight, outgate_weight),
        (
            expert_gate,
            expert_up,
            expert_down,
            shared_gate,
            shared_up,
            shared_down,
            ingate_weight.T,
            forget_weight.T,
            memory_state,
        ),
        capacity,
    )
    return publish(*results)


def solution(mesh):
    in_specs = (
        P("ep", None),
        P(),
        P(),
        P(),
        P(),
        P("ep", None),
        P("ep", None),
        P("ep", None),
        P("ep", None),
        P(),
        P(),
        P(),
        P(),
        P("ep", None, None, None),
        P("ep", None, None),
        P("ep", None),
        P(None, "ep"),
        P("ep", None),
        P("ep", None),
        P("ep", None, None),
        P("ep", None, None),
        P("ep", None, None),
        P(),
        P(),
        P(),
    )
    out_specs = (P("ep", None), P("ep", None, None, None), P("ep", None, None), P("ep", None))
    return jax.shard_map(
        on_device, mesh=mesh, in_specs=in_specs, out_specs=out_specs, check_vma=False
    )
```
